32 devices in a mesh: ep: 8 (over z, y), tp: 4 (over x, core).
Axes of the slice: x: 2, y: 2, z: 4, core: 2. Of those that a mesh axis runs over, the one named last changes fastest.
Arguments:
- tokens: bfloat16 [128, 1024], P('ep'), may hold values from -6 to 6
- attn_gain: float32 [1024], replicated, may hold values from 0.1 to 1.9
- q_down: bfloat16 [1024, 512], P(None, 'tp'), may hold values from -0.1875 to 0.1875
- kv_down: bfloat16 [1024, 512], P(None, 'tp'), may hold values from -0.1875 to 0.1875
- rope_down: bfloat16 [1024, 32], replicated, may hold values from -0.1875 to 0.1875
- q_latent_gain: float32 [512], replicated, may hold values from 0.1 to 1.9
- kv_latent_gain: float32 [512], replicated, may hold values from 0.1 to 1.9
- q_up: bfloat16 [512, 768], P(None, 'tp'), may hold values from -0.25 to 0.25
- query_gain: float32 [8, 96], P('tp'), may hold values from 0.4 to 48
- key_up: bfloat16 [512, 512], P(None, 'tp'), may hold values from -0.25 to 0.25
- value_up: bfloat16 [512, 512], P(None, 'tp'), may hold values from -0.25 to 0.25
- attn_out: bfloat16 [512, 1024], P('tp'), may hold values from -0.25 to 0.25
- cache_latent: bfloat16 [128, 512, 512], P(('ep', 'tp')), may hold values from -6 to 6
- cache_rope: bfloat16 [128, 32, 512], P(('ep', 'tp')), may hold values from -6 to 6
- lengths: int32 [128], P('ep'), may hold values from 1 to 512, as said below
- moe_gain: float32 [1024], replicated, may hold values from 0.1 to 1.9
- route: int32 [128, 6], P('ep'), may hold values from 0 to 7, as said below
- route_weight: float32 [128, 6], P('ep'), may hold values from 0.1 to 1
- expert_gate: bfloat16 [8, 1024, 512], P('ep', None, 'tp'), may hold values from -0.1875 to 0.1875
- expert_up: bfloat16 [8, 1024, 512], P('ep', None, 'tp'), may hold values from -0.1875 to 0.1875
- expert_down: bfloat16 [8, 512, 1024], P('ep', 'tp'), may hold values from -0.25 to 0.25
Outputs:
- mixed_out: bfloat16 [128, 1024], P('ep', 'tp')
- new_latent: bfloat16 [128, 512], P('ep', 'tp')
- new_rope: bfloat16 [128, 32], P('ep')
The draws below stay inside these ranges and needn't reach their ends.
Inputs may be any that keep to these rules, and one draw needn't show every extreme that they name: `route`: each row names 6 different experts that lie in one group of 8 consecutive expert numbers. Among the rows of the 16 sequences of one index of ep no expert is named more than 12 times, and some expert is named exactly 12 times by the rows of every index of ep. `lengths`: some sequence has exactly 512 cached positions.
All inputs are finite; a program needn't handle non-finite values.
Results may differ from the reference program's by a relative error of at most 0.02.
Values may be sent and summed in bfloat16 or wider, within the bound.
A program may use at most 64 MiB of HBM per device.

```python
import math
import jax
import jax.numpy as jnp
from jax import lax

D = 1024
HEADS = 8
NOPE = 64
ROPE = 32
VDIM = 64
QK = 96
Q_RANK = 512
KV_RANK = 512
FF = 512
EXPERTS = 8
EPG = 8
GROUPS = 1
TOPK = 6
SEQ_DEV = 16
CACHE_LEN = 512
SEQS = 128
NG_CAP = 16
CAP = 12
N_EP = 8
N_TP = 4


def draw_lengths(key, part):
    base_len = jax.random.randint(jax.random.fold_in(key, 11), (SEQS,), 1, CACHE_LEN + 1)
    longest = jax.random.randint(jax.random.fold_in(key, 12), (), 0, SEQS)
    return jnp.where(jnp.arange(SEQS) == longest, CACHE_LEN, base_len).astype(jnp.int32)


def draw_query_gain(key, part):
    noise = jax.random.truncated_normal(jax.random.fold_in(key, 23), -3.0, 3.0, (HEADS, QK), jnp.float32)
    return (1.0 + 0.18 * noise).astype(jnp.float32)


def draw_route(key, part):
    blocks_count = SEQS // SEQ_DEV
    slot_count = GROUPS * NG_CAP
    forced = jax.random.randint(jax.random.fold_in(key, 31), (), 0, GROUPS)
    forced_perm = jax.random.permutation(jax.random.fold_in(key, 32), EPG)
    slot_ids = jnp.arange(slot_count, dtype=jnp.int32)
    slot_group = slot_ids // NG_CAP
    noise = jax.random.randint(jax.random.fold_in(key, 33), (blocks_count, slot_count), 0, 1 << 16) * slot_count + slot_ids
    priority = jnp.where(slot_group[None, :] == forced, slot_ids[None, :] - slot_count, noise)
    chosen = jnp.argsort(priority, axis=1)[:, :SEQ_DEV]
    shuffle_keys = jax.random.randint(jax.random.fold_in(key, 34), (blocks_count, SEQ_DEV), 0, 1 << 16) * SEQ_DEV + jnp.arange(SEQ_DEV)
    taken = jnp.take_along_axis(chosen, jnp.argsort(shuffle_keys, axis=1), axis=1)
    groups_of = taken // NG_CAP
    ranks_of = taken % NG_CAP
    perm_keys = jax.random.randint(jax.random.fold_in(key, 35), (blocks_count, GROUPS, EPG), 0, 1 << 16) * EPG + jnp.arange(EPG)
    group_perm = jnp.argsort(perm_keys, axis=2)
    group_perm = jnp.where((jnp.arange(GROUPS) == forced)[None, :, None], forced_perm[None, None, :], group_perm)
    token_perm = group_perm[jnp.arange(blocks_count)[:, None], groups_of]
    offsets = (ranks_of[:, :, None] * TOPK + jnp.arange(TOPK)[None, None, :]) % EPG
    local_ids = jnp.take_along_axis(token_perm, offsets, axis=2)
    return (groups_of[:, :, None] * EPG + local_ids).reshape(SEQS, TOPK).astype(jnp.int32)


def block_levels(own_key, shape, shards, smallest, top_value):
    level, own = 1.0, jax.random.fold_in(own_key, 6)
    for dim, parts in shards:
        draws = jnp.exp(jax.random.uniform(jax.random.fold_in(own, dim), (parts,), jnp.float32, smallest / len(shards), top_value / len(shards)))
        level = level * jnp.repeat(draws, shape[dim] // parts).reshape([-1 if axis == dim else 1 for axis in range(len(shape))])
    return level


def normal_values(stream_key, shape, deviation, bound, cuts=(), kind=jnp.bfloat16):
    array = jax.random.normal(stream_key, shape, jnp.float32) * deviation
    if len(cuts) > 0:
        array = block_levels(stream_key, shape, cuts, -0.22, 0.18) * array
    return jnp.clip(array, min=-bound, max=bound).astype(kind)


def setup_inputs(seed: int = 0) -> dict:
    streams_of = jax.random.split(jax.random.key(seed), 22)
    tokens = normal_values(streams_of[0], (SEQS, D), 1.0, 6.0, ((0, 8),))
    attn_gain = jnp.clip(1.0 + 0.18 * jax.random.normal(streams_of[1], (D,), jnp.float32), 0.1, 1.9)
    q_down = normal_values(streams_of[2], (D, Q_RANK), D ** -0.5, 0.1875, ((1, 4),))
    kv_down = normal_values(streams_of[3], (D, KV_RANK), D ** -0.5, 0.1875, ((1, 4),))
    rope_down = normal_values(streams_of[4], (D, ROPE), D ** -0.5, 0.1875)
    q_latent_gain = jnp.clip(1.0 + 0.18 * jax.random.normal(streams_of[5], (Q_RANK,), jnp.float32), 0.1, 1.9)
    kv_latent_gain = jnp.clip(1.0 + 0.18 * jax.random.normal(streams_of[6], (KV_RANK,), jnp.float32), 0.1, 1.9)
    q_up = normal_values(streams_of[7], (Q_RANK, HEADS * QK), Q_RANK ** -0.5, 0.25, ((1, 4),))
    query_gain = draw_query_gain(jax.random.fold_in(streams_of[21], 71), 0)
    key_up = normal_values(streams_of[9], (KV_RANK, HEADS * NOPE), KV_RANK ** -0.5, 0.25, ((1, 4),))
    value_up = normal_values(streams_of[10], (KV_RANK, HEADS * VDIM), KV_RANK ** -0.5, 0.25, ((1, 4),))
    attn_out = normal_values(streams_of[11], (HEADS * VDIM, D), (HEADS * VDIM) ** -0.5, 0.25, ((0, 4),))
    cache_latent = normal_values(streams_of[12], (SEQS, CACHE_LEN, KV_RANK), 1.0, 6.0, ((0, 32),))
    cache_rope = normal_values(streams_of[13], (SEQS, ROPE, CACHE_LEN), 1.0, 6.0, ((0, 32),))
    lengths = draw_lengths(jax.random.fold_in(streams_of[21], 71), 0)
    moe_gain = jnp.clip(1.0 + 0.18 * jax.random.normal(streams_of[15], (D,), jnp.float32), 0.1, 1.9)
    route = draw_route(jax.random.fold_in(streams_of[21], 71), 0)
    route_weight = jnp.clip(jnp.exp(math.log(1.0) - 2.3025851 * jax.random.uniform(streams_of[17], (SEQS, TOPK), jnp.float32) ** block_levels(streams_of[17], (SEQS, TOPK), ((0, 8),), -0.2, 0.2)), 0.1, 1.0)
    expert_gate = normal_values(streams_of[18], (EXPERTS, D, FF), D ** -0.5, 0.1875, ((0, 8), (2, 4)))
    expert_up = normal_values(streams_of[19], (EXPERTS, D, FF), D ** -0.5, 0.1875, ((0, 8), (2, 4)))
    expert_down = normal_values(streams_of[20], (EXPERTS, FF, D), FF ** -0.5, 0.25, ((0, 8), (1, 4)))
    return {"tokens": tokens, "attn_gain": attn_gain, "q_down": q_down, "kv_down": kv_down, "rope_down": rope_down, "q_latent_gain": q_latent_gain, "kv_latent_gain": kv_latent_gain, "q_up": q_up, "query_gain": query_gain, "key_up": key_up, "value_up": value_up, "attn_out": attn_out, "cache_latent": cache_latent, "cache_rope": cache_rope, "lengths": lengths, "moe_gain": moe_gain, "route": route, "route_weight": route_weight, "expert_gate": expert_gate, "expert_up": expert_up, "expert_down": expert_down}


EPS = 1e-06
ROPE_BASE = 10000.0

def rms_scaled(values_in, gain_vec):
    values_in = values_in.astype(jnp.float32)
    return values_in * lax.rsqrt(lax.optimization_barrier(jnp.mean(values_in * values_in, axis=-1, keepdims=True)) + EPS) * gain_vec

def rotate_last(values_in, positions):
    half_dim = values_in.shape[-1] // 2
    inverse = ROPE_BASE ** (-jnp.arange(half_dim, dtype=jnp.float32) / half_dim)
    angles = positions.astype(jnp.float32)[..., None] * inverse
    lower_half = values_in[..., :half_dim]
    upper_half = values_in[..., half_dim:]
    return jnp.concatenate([lower_half * jnp.cos(angles) - upper_half * jnp.sin(angles), upper_half * jnp.cos(angles) + lower_half * jnp.sin(angles)], -1)

def rotate_rows(values_in, positions):
    half_dim = values_in.shape[1] // 2
    inverse = ROPE_BASE ** (-jnp.arange(half_dim, dtype=jnp.float32) / half_dim)
    angles = inverse[:, None] * positions.astype(jnp.float32)[None, :]
    lower_half = values_in[:, :half_dim]
    upper_half = values_in[:, half_dim:]
    return jnp.concatenate([lower_half * jnp.cos(angles) - upper_half * jnp.sin(angles), upper_half * jnp.cos(angles) + lower_half * jnp.sin(angles)], 1)

def reference(tokens, attn_gain, q_down, kv_down, rope_down, q_latent_gain, kv_latent_gain, q_up, query_gain, key_up, value_up, attn_out, cache_latent, cache_rope, lengths, moe_gain, route, route_weight, expert_gate, expert_up, expert_down):
    score_scale = QK ** (-0.5)
    normed = rms_scaled(tokens, attn_gain).astype(jnp.bfloat16)
    q_raw = jnp.dot(normed, q_down, preferred_element_type=jnp.float32).astype(jnp.bfloat16)
    kv_raw = jnp.dot(normed, kv_down, preferred_element_type=jnp.float32).astype(jnp.bfloat16)
    new_rope = jnp.dot(normed, rope_down, preferred_element_type=jnp.float32).astype(jnp.bfloat16)
    q_lat = rms_scaled(q_raw, q_latent_gain).astype(jnp.bfloat16)
    new_latent = rms_scaled(kv_raw, kv_latent_gain).astype(jnp.bfloat16)
    query_head = rms_scaled(jnp.dot(q_lat, q_up, preferred_element_type=jnp.float32).reshape(SEQS, HEADS, QK), query_gain)
    query_head = jnp.concatenate([query_head[..., :NOPE], rotate_last(query_head[..., NOPE:], lengths[:, None])], -1).astype(jnp.bfloat16)
    absorbed = jnp.einsum('shn,rhn->shr', query_head[..., :NOPE].astype(jnp.float32), key_up.reshape(KV_RANK, HEADS, NOPE).astype(jnp.float32)).astype(jnp.bfloat16)
    rot_query = query_head[..., NOPE:]
    key_new = rotate_last(new_rope.astype(jnp.float32), lengths).astype(jnp.bfloat16)
    self_score = (jnp.einsum('shr,sr->sh', absorbed.astype(jnp.float32), new_latent.astype(jnp.float32)) + jnp.einsum('shp,sp->sh', rot_query.astype(jnp.float32), key_new.astype(jnp.float32))) * score_scale

    def attend(block_data):
        absorbed_b, rot_b, cache_b, rope_b, len_b, self_b, latent_b = block_data
        positions = jnp.arange(CACHE_LEN, dtype=jnp.int32)
        rotated_keys = rotate_rows(rope_b.astype(jnp.float32), positions).astype(jnp.bfloat16)
        scores = (jnp.einsum('shr,sjr->shj', absorbed_b.astype(jnp.float32), cache_b.astype(jnp.float32)) + jnp.einsum('shp,spj->shj', rot_b.astype(jnp.float32), rotated_keys.astype(jnp.float32))) * score_scale
        valid_keys = positions[None, :] < len_b[:, None]
        masked = jnp.where(valid_keys[:, None, :], scores, -jnp.inf)
        row_max = jnp.maximum(lax.optimization_barrier(jnp.max(masked, axis=-1)), self_b)
        weights = jnp.exp(masked - row_max[..., None])
        self_weight = jnp.exp(self_b - row_max)
        total_weight = lax.optimization_barrier(jnp.sum(weights, axis=-1)) + self_weight
        latent_sum = jnp.einsum('shj,sjr->shr', weights.astype(jnp.bfloat16).astype(jnp.float32), cache_b.astype(jnp.float32))
        latent_sum = latent_sum + self_weight.astype(jnp.bfloat16).astype(jnp.float32)[..., None] * latent_b.astype(jnp.float32)[:, None, :]
        return (latent_sum / total_weight[..., None]).astype(jnp.bfloat16)

    def split_seqs(array_in):
        return array_in.reshape((SEQS // SEQ_DEV, SEQ_DEV) + array_in.shape[1:])
    attended = lax.map(attend, tuple((split_seqs(a) for a in (absorbed, rot_query, cache_latent, cache_rope, lengths, self_score, new_latent))))
    attended = attended.reshape(SEQS, HEADS, KV_RANK)
    head_values = jnp.einsum('shr,rhv->shv', attended.astype(jnp.float32), value_up.reshape(KV_RANK, HEADS, VDIM).astype(jnp.float32)).astype(jnp.bfloat16)
    group_cols = HEADS * VDIM // N_TP
    partials = jnp.einsum('sgk,gkd->gsd', head_values.reshape(SEQS, N_TP, group_cols).astype(jnp.float32), attn_out.reshape(N_TP, group_cols, D).astype(jnp.float32))
    head_sum = lax.optimization_barrier(jnp.sum(partials.astype(jnp.bfloat16).astype(jnp.float32), axis=0))
    attn_resid = (tokens.astype(jnp.float32) + head_sum).astype(jnp.bfloat16)
    moe_input = rms_scaled(attn_resid, moe_gain).astype(jnp.bfloat16)
    rows_dev = SEQ_DEV * TOPK
    route_blocks = route.reshape(N_EP, rows_dev)
    same_expert = route_blocks[:, :, None] == route_blocks[:, None, :]
    earlier = jnp.arange(rows_dev)[None, :] < jnp.arange(rows_dev)[:, None]
    slot_rank = lax.optimization_barrier(jnp.sum(same_expert & earlier[None], axis=-1)).astype(jnp.int32)
    slot_index = (jnp.arange(N_EP, dtype=jnp.int32)[:, None] * CAP + slot_rank).reshape(-1)
    flat_route = route.reshape(-1)
    buffer = jnp.zeros((EXPERTS, N_EP * CAP, D), jnp.bfloat16).at[flat_route, slot_index].set(jnp.repeat(moe_input, TOPK, axis=0))

    def expert(block_data):
        row_data, gate_weight, up_weight, down_weight = block_data
        gate_pre = jnp.dot(row_data, gate_weight, preferred_element_type=jnp.float32)
        up_pre = jnp.dot(row_data, up_weight, preferred_element_type=jnp.float32)
        hidden = (jax.nn.silu(gate_pre) * up_pre).astype(jnp.bfloat16)
        ff_part = FF // N_TP
        partial_value = jnp.einsum('rgf,gfd->grd', hidden.reshape(-1, N_TP, ff_part).astype(jnp.float32), down_weight.reshape(N_TP, ff_part, D).astype(jnp.float32))
        return lax.optimization_barrier(jnp.sum(partial_value.astype(jnp.bfloat16).astype(jnp.float32), axis=0)).astype(jnp.bfloat16)
    outputs = lax.map(expert, (buffer, expert_gate, expert_up, expert_down))
    picked = outputs[flat_route, slot_index].astype(jnp.float32).reshape(SEQS, TOPK, D)
    mixed_out = (attn_resid.astype(jnp.float32) + lax.optimization_barrier(jnp.sum(picked * route_weight[..., None], axis=1))).astype(jnp.bfloat16)
    return (mixed_out, new_latent, new_rope)
```

```python
import functools
import math

import jax
import jax.numpy as jnp
from jax import lax
from jax.experimental import pallas as pl
from jax.experimental.pallas import tpu as pltpu
from jax.sharding import PartitionSpec as P

NOPE = 64
EPS = 1e-06
ROPE_BASE = 10000.0
MESH = pl.DeviceIdType.MESH
BF = jnp.bfloat16
F32 = jnp.float32


def shift_of(n):
    s = n.bit_length() - 1
    assert 1 << s == n
    return s


def div(v, n):
    return lax.shift_right_logical(v, jnp.int32(shift_of(n)))


def mod(v, n):
    return jnp.bitwise_and(v, jnp.int32(n - 1))


def iota(shape, dim):
    return lax.broadcasted_iota(jnp.int32, shape, dim)


def mm(a, b):
    return jnp.dot(a, b, preferred_element_type=F32)


def mm_nt(a, b):
    return lax.dot_general(a, b, (((1,), (1,)), ((), ())), preferred_element_type=F32)


def exact(a, b):
    return jnp.dot(a, b, preferred_element_type=F32, precision=lax.Precision.HIGHEST)


def kernel(
    ep_n,
    tp_n,
    tokens,
    attn_gain,
    q_down_h,
    kv_down_h,
    rope_down_h,
    q_gain,
    kv_gain,
    q_up_h,
    query_gain,
    key_up_h,
    value_up_h,
    attn_out_h,
    cache_h,
    rope_h,
    lengths,
    moe_gain,
    route,
    route_weight,
    gate_h,
    up_h,
    down_h,
    mixed_ref,
    latent_ref,
    rope_ref,
    q_down,
    kv_down,
    rope_down,
    q_up,
    key_up,
    value_up,
    attn_out,
    cache,
    crope,
    gate_w,
    up_w,
    down_w,
    lat_buf,
    query_out,
    query_in,
    att_out,
    att_in,
    sum_out,
    sum_in,
    rows_in,
    part_out,
    part_in,
    load_sem,
    tp_send,
    tp_recv,
    all_send,
    all_recv,
):
    ep_me = lax.axis_index("ep")
    me = lax.axis_index("tp")
    n = ep_n * tp_n
    lin = ep_me * tp_n + me
    seqs = tokens.shape[0]
    cols = tokens.shape[1] // tp_n
    heads, qk = query_gain.shape
    ropes = qk - NOPE
    half = ropes // 2
    s_here = cache.shape[0]
    rank = cache.shape[2]
    rows = tp_n * heads * s_here
    block = heads * s_here
    lanes = 128

    loads = [
        pltpu.make_async_copy(src, dst, load_sem.at[i])
        for i, (src, dst) in enumerate(
            [
                (q_down_h, q_down),
                (kv_down_h, kv_down),
                (rope_down_h, rope_down),
                (q_up_h, q_up),
                (key_up_h, key_up),
                (rope_h, crope),
                (cache_h, cache),
                (value_up_h, value_up),
                (attn_out_h, attn_out),
                (gate_h, gate_w),
                (up_h, up_w),
                (down_h, down_w),
            ]
        )
    ]
    for load in loads:
        load.start()

    barrier = pltpu.get_barrier_semaphore()

    def greet(k, carry):
        to = lax.rem(lin + k, n)
        pl.semaphore_signal(barrier, inc=1, device_id=(to // tp_n, lax.rem(to, tp_n)), device_id_type=MESH)
        return carry

    lax.fori_loop(1, n, greet, 0)

    def tp_copy(stage, src, dst, to, origin):
        return pltpu.make_async_remote_copy(
            src_ref=src,
            dst_ref=dst,
            send_sem=tp_send.at[stage, to],
            recv_sem=tp_recv.at[stage, origin],
            device_id=(ep_me, to),
            device_id_type=MESH,
        )

    def exchange(stage, src_of, dst_of):
        for k in range(1, tp_n):
            to = lax.rem(me + k, tp_n)
            tp_copy(stage, src_of(to), dst_of(me), to, me).start()

    def arrive(stage, src_of, dst_of):
        for k in range(1, tp_n):
            other = lax.rem(me + k, tp_n)
            tp_copy(stage, src_of(other), dst_of(other), other, other).wait_recv()

    def sent(stage, src_of, dst_of):
        for k in range(1, tp_n):
            other = lax.rem(me + k, tp_n)
            tp_copy(stage, src_of(other), dst_of(other), other, other).wait_send()

    tok = tokens[...].astype(F32)
    normed = (tok * lax.rsqrt(jnp.mean(tok * tok, axis=-1, keepdims=True) + EPS) * attn_gain[...]).astype(BF)
    loads[0].wait()
    qc = q_down.shape[1]
    kc = kv_down.shape[1]
    q_part = mm(normed, q_down[...]).astype(BF)
    loads[1].wait()
    kv_part = mm(normed, kv_down[...]).astype(BF)
    lat_buf[me, :, :qc] = q_part
    lat_buf[me, :, qc:] = kv_part
    pl.semaphore_wait(barrier, n - 1)
    own_lat = lambda to: lat_buf.at[me]
    lat_at = lambda i: lat_buf.at[i]
    exchange(0, own_lat, lat_at)

    loads[2].wait()
    new_rope = mm(normed, rope_down[...]).astype(BF)
    rope_ref[...] = new_rope
    len_row = lengths[...].astype(F32)
    eye = iota((seqs, seqs), 0) == iota((seqs, seqs), 1)
    len_col = jnp.sum(jnp.where(eye, len_row, 0.0), axis=1, keepdims=True)
    lane1 = iota((1, lanes), 1)
    inv_lane = jnp.exp(mod(lane1, half).astype(F32) * (-math.log(ROPE_BASE) / half))
    ang = len_col * inv_lane
    cos_q, sin_q = jnp.cos(ang), jnp.sin(ang)

    width = heads * qk
    src_i, out_c = iota((width, lanes), 0), iota((width, lanes), 1)
    pick_n = jnp.where(src_i == div(out_c, NOPE) * qk + mod(out_c, NOPE), 1.0, 0.0).astype(BF)
    rope_head, rope_p = div(out_c, ropes), mod(out_c, ropes)
    live = out_c < heads * ropes
    pick_a = jnp.where(live & (src_i == rope_head * qk + NOPE + rope_p), 1.0, 0.0)
    pick_b = jnp.where(
        live & (src_i == rope_head * qk + NOPE + mod(rope_p + half, ropes)),
        jnp.where(rope_p < half, -1.0, 1.0),
        0.0,
    )
    key_i, key_c = iota((ropes, lanes), 0), iota((ropes, lanes), 1)
    key_p = mod(key_c, ropes)
    key_a = jnp.where(key_i == key_p, 1.0, 0.0).astype(BF)
    key_b = jnp.where(key_i == mod(key_p + half, ropes), jnp.where(key_p < half, -1.0, 1.0), 0.0).astype(BF)
    key_new = (mm(new_rope, key_a) * cos_q + mm(new_rope, key_b) * sin_q).astype(BF)

    g_i, g_c = iota((qk, width), 0), iota((qk, width), 1)
    tile = jnp.zeros((qk, width), F32)
    for h in range(heads):
        tile = jnp.where(g_c - h * qk == g_i, 1.0, tile)
    gains = exact(query_gain[...], tile)
    lane_w = iota((1, width), 1)
    gain = gains[0:1]
    for h in range(1, heads):
        gain = jnp.where(lane_w >= h * qk, gains[h : h + 1], gain)

    row_i, seq_c = iota((rows, seqs), 0), iota((rows, seqs), 1)
    spread = jnp.where(div(row_i, block) * s_here + mod(row_i, s_here) == seq_c, 1.0, 0.0).astype(BF)
    mine_mask = me * s_here + mod(row_i, s_here) == seq_c
    mine = jnp.where(mine_mask, 1.0, 0.0).astype(BF)
    len_rows = jnp.sum(jnp.where(mine_mask, len_row, 0.0), axis=1, keepdims=True)
    row_l, lane_l = iota((rows, lanes), 0), iota((rows, lanes), 1)
    row_head = mod(div(row_l, s_here), heads)
    head_lanes = div(lane_l, NOPE) == row_head
    rope_lanes = div(lane_l, ropes) == row_head

    loads[5].wait()
    positions = crope.shape[2]
    inv_sub = jnp.exp(iota((half, positions), 0).astype(F32) * (-math.log(ROPE_BASE) / half))
    kang = inv_sub * iota((half, positions), 1).astype(F32)
    kcos, ksin = jnp.cos(kang), jnp.sin(kang)
    rotated = []
    pad = jnp.zeros((lanes - heads * ropes, positions), BF)
    for s in range(s_here):
        u = crope[s, :half, :].astype(F32)
        w = crope[s, half:, :].astype(F32)
        a = (u * kcos - w * ksin).astype(BF)
        b = (w * kcos + u * ksin).astype(BF)
        rotated.append(jnp.concatenate([a, b] * heads + [pad], axis=0))

    arrive(0, own_lat, lat_at)
    q_raw = jnp.concatenate([lat_buf[t, :, :qc] for t in range(tp_n)], axis=1).astype(F32)
    kv_raw = jnp.concatenate([lat_buf[t, :, qc:] for t in range(tp_n)], axis=1).astype(F32)
    q_lat = (q_raw * lax.rsqrt(jnp.mean(q_raw * q_raw, axis=-1, keepdims=True) + EPS) * q_gain[...]).astype(BF)
    loads[3].wait()
    query = mm(q_lat, q_up[...])
    scale = jnp.zeros_like(query)
    lane_q = iota(query.shape, 1)
    for h in range(heads):
        inside = (lane_q >= h * qk) & (lane_q < (h + 1) * qk)
        total = jnp.sum(jnp.where(inside, query * query, 0.0), axis=-1, keepdims=True)
        scale = jnp.where(inside, lax.rsqrt(total * (1.0 / qk) + EPS), scale)
    query = query * scale * gain
    nope = mm(query.astype(BF), pick_n).astype(BF)
    rot = (exact(query, pick_a) * cos_q + exact(query, pick_b) * sin_q).astype(BF)
    nope_rows = jnp.where(head_lanes, mm(spread, nope), 0.0).astype(BF)
    rot_rows = jnp.where(rope_lanes, mm(spread, rot), 0.0).astype(BF)
    loads[4].wait()
    absorbed = mm_nt(nope_rows, key_up[...]).astype(BF)
    for t in range(tp_n):
        query_out[t, :, :rank] = absorbed[t * block : (t + 1) * block]
        query_out[t, :, rank:] = rot_rows[t * block : (t + 1) * block]
    q_src = lambda to: query_out.at[to]
    q_dst = lambda i: query_in.at[i]
    exchange(1, q_src, q_dst)
    query_in[me] = query_out[me]

    kv_scale = lax.rsqrt(jnp.mean(kv_raw * kv_raw, axis=-1, keepdims=True) + EPS)
    latent_new = (kv_raw * kv_scale * kv_gain[...]).astype(BF)
    own_cols = pl.ds(pl.multiple_of(me * kc, kc), kc)
    latent_ref[...] = (kv_part.astype(F32) * kv_scale * kv_gain[:, own_cols]).astype(BF)
    latent_rows = mm(mine, latent_new)
    key_rows = mm(mine, key_new)
    loads[6].wait()

    arrive(1, q_src, q_dst)
    q_abs = jnp.concatenate([query_in[t, :, :rank] for t in range(tp_n)], axis=0)
    q_rot = jnp.concatenate([query_in[t, :, rank:] for t in range(tp_n)], axis=0)
    row_p, pos_p = iota((rows, positions), 0), iota((rows, positions), 1)
    row_seq = mod(row_p, s_here)
    scores = jnp.zeros((rows, positions), F32)
    for s in range(s_here):
        scores = jnp.where(row_seq == s, mm_nt(q_abs, cache[s]) + mm(q_rot, rotated[s]), scores)
    score_scale = qk ** (-0.5)
    scores = scores * score_scale
    self_score = (
        jnp.sum(q_abs.astype(F32) * latent_rows, axis=-1, keepdims=True)
        + jnp.sum(q_rot.astype(F32) * key_rows, axis=-1, keepdims=True)
    ) * score_scale
    valid = pos_p.astype(F32) < len_rows
    scores = jnp.where(valid, scores, -jnp.inf)
    top = jnp.maximum(jnp.max(scores, axis=-1, keepdims=True), self_score)
    weights = jnp.exp(scores - top)
    self_weight = jnp.exp(self_score - top)
    total = jnp.sum(weights, axis=-1, keepdims=True) + self_weight
    acc = self_weight.astype(BF).astype(F32) * latent_rows
    for s in range(s_here):
        acc = acc + mm(jnp.where(row_seq == s, weights, 0.0).astype(BF), cache[s])
    attended = (acc / total).astype(BF)
    for t in range(tp_n):
        att_out[t] = attended[t * block : (t + 1) * block]
    a_src = lambda to: att_out.at[to]
    a_dst = lambda i: att_in.at[i]
    exchange(2, a_src, a_dst)
    att_in[me] = att_out[me]
    loads[7].wait()
    loads[8].wait()
    seq_i, row_c = iota((seqs, rows), 0), iota((seqs, rows), 1)
    gather = jnp.where(div(row_c, block) * s_here + mod(row_c, s_here) == seq_i, 1.0, 0.0).astype(BF)

    arrive(2, a_src, a_dst)
    att = jnp.concatenate([att_in[t] for t in range(tp_n)], axis=0)
    values = jnp.where(head_lanes, mm(att, value_up[...]), 0.0).astype(BF)
    head_values = mm(gather, values).astype(BF)
    partial = mm(head_values, attn_out[...]).astype(BF)
    for t in range(tp_n):
        sum_out[t] = partial[:, t * cols : (t + 1) * cols]
    s_src = lambda to: sum_out.at[to]
    s_dst = lambda i: sum_in.at[i]
    exchange(3, s_src, s_dst)
    sum_in[me] = sum_out[me]
    model_cols = pl.ds(pl.multiple_of(me * cols, cols), cols)
    tok_mine = tokens[:, model_cols].astype(F32)
    loads[9].wait()
    loads[10].wait()
    loads[11].wait()

    arrive(3, s_src, s_dst)
    head_sum = sum_in[0].astype(F32)
    for t in range(1, tp_n):
        head_sum = head_sum + sum_in[t].astype(F32)
    resid = (tok_mine + head_sum).astype(BF)
    rows_in[lin] = resid

    def all_copy(stage, src, dst, to):
        return pltpu.make_async_remote_copy(
            src_ref=src,
            dst_ref=dst,
            send_sem=all_send.at[stage],
            recv_sem=all_recv.at[stage],
            device_id=(to // tp_n, lax.rem(to, tp_n)),
            device_id_type=MESH,
        )

    def give_rows(k, carry):
        to = lax.rem(lin + k, n)
        all_copy(0, rows_in.at[lin], rows_in.at[lin], to).start()
        return carry

    lax.fori_loop(1, n, give_rows, 0)

    def all_wait(stage, src, dst):
        others = pl.ds(0, n - 1)
        return all_copy(stage, src.at[others], dst.at[others], lax.rem(lin + 1, n))

    all_wait(0, rows_in, rows_in).wait_recv()

    group = math.gcd(ep_n, 8)

    def expert(g, carry):
        first = g * group
        parts = []
        square = jnp.zeros((group * seqs, 1), F32)
        for t in range(tp_n):
            x = jnp.concatenate([rows_in[(first + i) * tp_n + t] for i in range(group)], axis=0).astype(F32)
            square = square + jnp.sum(x * x, axis=-1, keepdims=True)
            parts.append(x)
        inverse = lax.rsqrt(square * (1.0 / (cols * tp_n)) + EPS)
        gate = jnp.zeros((group * seqs, gate_w.shape[2]), F32)
        up = jnp.zeros((group * seqs, gate_w.shape[2]), F32)
        for t in range(tp_n):
            here = slice(t * cols, (t + 1) * cols)
            x = (parts[t] * inverse * moe_gain[:, here]).astype(BF)
            gate = gate + mm(x, gate_w[0, here, :])
            up = up + mm(x, up_w[0, here, :])
        hidden = (gate / (1.0 + jnp.exp(-gate)) * up).astype(BF)
        for t in range(tp_n):
            here = slice(t * cols, (t + 1) * cols)
            part = mm(hidden, down_w[0, :, here]).astype(BF)
            for i in range(group):
                part_out[(first + i) * tp_n + t] = part[i * seqs : (i + 1) * seqs]
        return carry

    if ep_n == group:
        expert(0, 0)
    else:
        lax.fori_loop(0, ep_n // group, expert, 0)

    def give_parts(k, carry):
        to = lax.rem(lin + k, n)
        all_copy(1, part_out.at[to], part_in.at[lin], to).start()
        return carry

    lax.fori_loop(1, n, give_parts, 0)
    part_in[lin] = part_out[lin]
    chosen = route[...]
    chosen_weight = route_weight[...]
    all_wait(1, part_out, part_in).wait_recv()

    def combine(e, mixed):
        found = part_in[e * tp_n].astype(F32)
        for t in range(1, tp_n):
            found = found + part_in[e * tp_n + t].astype(F32)
        share = jnp.sum(jnp.where(chosen == e, chosen_weight, 0.0), axis=1, keepdims=True)
        return mixed + share * found.astype(BF).astype(F32)

    mixed = jnp.zeros((seqs, cols), F32)
    if ep_n <= 8:
        for e in range(ep_n):
            mixed = combine(e, mixed)
    else:
        mixed = lax.fori_loop(0, ep_n, combine, mixed)
    mixed_ref[...] = (resid.astype(F32) + mixed).astype(BF)

    sent(0, own_lat, lat_at)
    sent(1, q_src, q_dst)
    sent(2, a_src, a_dst)
    sent(3, s_src, s_dst)
    all_wait(0, rows_in, rows_in).wait_send()
    all_wait(1, part_out, part_in).wait_send()


def shards(ep_n, tp_n, *args):
    (
        tokens,
        attn_gain,
        q_down,
        kv_down,
        rope_down,
        q_latent_gain,
        kv_latent_gain,
        q_up,
        query_gain,
        key_up,
        value_up,
        attn_out,
        cache_latent,
        cache_rope,
        lengths,
        moe_gain,
        route,
        route_weight,
        expert_gate,
        expert_up,
        expert_down,
    ) = args
    assert expert_gate.shape[0] == 1
    row = lambda v: v.reshape(1, -1)
    operands = (
        tokens,
        row(attn_gain),
        q_down,
        kv_down,
        rope_down,
        row(q_latent_gain),
        row(kv_latent_gain),
        q_up,
        query_gain,
        key_up,
        value_up,
        attn_out,
        cache_latent,
        cache_rope,
        row(lengths),
        row(moe_gain),
        route,
        route_weight,
        expert_gate,
        expert_up,
        expert_down,
    )
    far = {2, 3, 4, 7, 9, 10, 11, 12, 13, 18, 19, 20}
    vmem = pl.BlockSpec(memory_space=pltpu.VMEM)
    anyspace = pl.BlockSpec(memory_space=pl.ANY)
    seqs, model = tokens.shape
    cols = model // tp_n
    n = ep_n * tp_n
    heads = query_gain.shape[0]
    s_here, _, rank = cache_latent.shape
    block = heads * s_here
    like = lambda v: pltpu.VMEM(v.shape, v.dtype)
    scratch = [
        like(q_down),
        like(kv_down),
        like(rope_down),
        like(q_up),
        like(key_up),
        like(value_up),
        like(attn_out),
        like(cache_latent),
        like(cache_rope),
        like(expert_gate),
        like(expert_up),
        like(expert_down),
        pltpu.VMEM((tp_n, seqs, q_down.shape[1] + kv_down.shape[1]), BF),
        pltpu.VMEM((tp_n, block, rank + 128), BF),
        pltpu.VMEM((tp_n, block, rank + 128), BF),
        pltpu.VMEM((tp_n, block, rank), BF),
        pltpu.VMEM((tp_n, block, rank), BF),
        pltpu.VMEM((tp_n, seqs, cols), BF),
        pltpu.VMEM((tp_n, seqs, cols), BF),
        pltpu.VMEM((n, seqs, cols), BF),
        pltpu.VMEM((n, seqs, cols), BF),
        pltpu.VMEM((n, seqs, cols), BF),
        pltpu.SemaphoreType.DMA((12,)),
        pltpu.SemaphoreType.DMA((4, tp_n)),
        pltpu.SemaphoreType.DMA((4, tp_n)),
        pltpu.SemaphoreType.DMA((2,)),
        pltpu.SemaphoreType.DMA((2,)),
    ]
    return pl.pallas_call(
        functools.partial(kernel, ep_n, tp_n),
        out_shape=(
            jax.ShapeDtypeStruct((seqs, cols), BF),
            jax.ShapeDtypeStruct((seqs, kv_down.shape[1]), BF),
            jax.ShapeDtypeStruct((seqs, rope_down.shape[1]), BF),
        ),
        in_specs=[anyspace if i in far else vmem for i in range(len(operands))],
        out_specs=(vmem, vmem, vmem),
        scratch_shapes=scratch,
        compiler_params=pltpu.CompilerParams(
            collective_id=0, has_side_effects=True, vmem_limit_bytes=60 * 1024 * 1024
        ),
    )(*operands)


def solution(mesh):
    placed = (
        P("ep", None),
        P(),
        P(None, "tp"),
        P(None, "tp"),
        P(),
        P(),
        P(),
        P(None, "tp"),
        P("tp", None),
        P(None, "tp"),
        P(None, "tp"),
        P("tp", None),
        P(("ep", "tp"), None, None),
        P(("ep", "tp"), None, None),
        P("ep"),
        P(),
        P("ep", None),
        P("ep", None),
        P("ep", None, "tp"),
        P("ep", None, "tp"),
        P("ep", "tp", None),
    )
    return jax.shard_map(
        functools.partial(shards, mesh.shape["ep"], mesh.shape["tp"]),
        mesh=mesh,
        in_specs=placed,
        out_specs=(P("ep", "tp"), P("ep", "tp"), P("ep", None)),
        check_vma=False,
    )
```

```python
import functools
import math

import jax
import jax.numpy as jnp
from jax import lax
from jax.experimental import pallas as pl
from jax.experimental.pallas import tpu as pltpu
from jax.sharding import PartitionSpec as P

NOPE = 64
EPS = 1e-06
ROPE_BASE = 10000.0
MESH = pl.DeviceIdType.MESH
BF = jnp.bfloat16
F32 = jnp.float32


def shift_of(n):
    s = n.bit_length() - 1
    assert 1 << s == n
    return s


def div(v, n):
    return lax.shift_right_logical(v, jnp.int32(shift_of(n)))


def mod(v, n):
    return jnp.bitwise_and(v, jnp.int32(n - 1))


def iota(shape, dim):
    return lax.broadcasted_iota(jnp.int32, shape, dim)


def mm(a, b):
    return jnp.dot(a, b, preferred_element_type=F32)


def mm_nt(a, b):
    return lax.dot_general(a, b, (((1,), (1,)), ((), ())), preferred_element_type=F32)


def exact(a, b):
    return jnp.dot(a, b, preferred_element_type=F32, precision=lax.Precision.HIGHEST)


def kernel(ep_n, tp_n, count, *refs):
    far = refs[:count]
    mixed_ref, latent_ref, rope_ref = refs[count : count + 3]
    near = refs[count + 3 : 2 * count + 3]
    (
        tokens,
        attn_gain,
        q_down,
        kv_down,
        rope_down,
        q_gain,
        kv_gain,
        q_up,
        query_gain,
        key_up,
        value_up,
        attn_out,
        cache,
        crope,
        lengths,
        moe_gain,
        route,
        route_weight,
        gate_w,
        up_w,
        down_w,
    ) = near
    (
        lat_buf,
        query_out,
        query_in,
        att_out,
        att_in,
        sum_out,
        sum_in,
        rows_in,
        part_out,
        part_in,
        back_out,
        back_in,
        load_sem,
        tp_send,
        tp_recv,
        rows_recv,
        part_recv,
        bulk,
    ) = refs[2 * count + 3 :]
    ep_me = lax.axis_index("ep")
    me = lax.axis_index("tp")
    seqs = tokens.shape[0]
    cols = tokens.shape[1] // tp_n
    heads, qk = query_gain.shape
    ropes = qk - NOPE
    half = ropes // 2
    s_here = cache.shape[0]
    rank = cache.shape[2]
    rows = tp_n * heads * s_here
    block = heads * s_here
    lanes = 128

    loads = [pltpu.make_async_copy(far[i], near[i], load_sem.at[i]) for i in range(count)]
    for i in (0, 1, 2, 3, 4, 14, 5, 6, 7, 8, 9, 13, 12, 10, 11, 15, 16, 17, 18, 19, 20):
        loads[i].start()

    barrier = pltpu.get_barrier_semaphore()
    for k in range(1, tp_n):
        pl.semaphore_signal(barrier, inc=1, device_id=(ep_me, lax.rem(me + k, tp_n)), device_id_type=MESH)

    def greet(k, carry):
        pl.semaphore_signal(barrier, inc=1, device_id=(lax.rem(ep_me + k, ep_n), me), device_id_type=MESH)
        return carry

    lax.fori_loop(1, ep_n, greet, 0)

    def tp_copy(stage, src, dst, to, origin):
        return pltpu.make_async_remote_copy(
            src_ref=src,
            dst_ref=dst,
            send_sem=tp_send.at[stage, to],
            recv_sem=tp_recv.at[stage, origin],
            device_id=(ep_me, to),
            device_id_type=MESH,
        )

    def exchange(stage, src_of, dst_of):
        for k in range(1, tp_n):
            to = lax.rem(me + k, tp_n)
            tp_copy(stage, src_of(to), dst_of(me), to, me).start()

    def arrive(stage, src_of, dst_of):
        for k in range(1, tp_n):
            other = lax.rem(me + k, tp_n)
            tp_copy(stage, src_of(other), dst_of(other), other, other).wait_recv()

    def sent(stage, src_of, dst_of):
        for k in range(1, tp_n):
            other = lax.rem(me + k, tp_n)
            tp_copy(stage, src_of(other), dst_of(other), other, other).wait_send()

    loads[0].wait()
    loads[1].wait()
    tok = tokens[...].astype(F32)
    normed = (tok * lax.rsqrt(jnp.mean(tok * tok, axis=-1, keepdims=True) + EPS) * attn_gain[...]).astype(BF)
    loads[2].wait()
    qc = q_down.shape[1]
    kc = kv_down.shape[1]
    q_part = mm(normed, q_down[...]).astype(BF)
    loads[3].wait()
    kv_part = mm(normed, kv_down[...]).astype(BF)
    lat_buf[me, :, :qc] = q_part
    lat_buf[me, :, qc:] = kv_part
    pl.semaphore_wait(barrier, ep_n + tp_n - 2)
    own_lat = lambda to: lat_buf.at[me]
    lat_at = lambda i: lat_buf.at[i]
    exchange(0, own_lat, lat_at)

    loads[4].wait()
    loads[14].wait()
    new_rope = mm_nt(normed, rope_down[...]).astype(BF)
    rope_ref[...] = new_rope
    len_row = lengths[...].astype(F32)
    eye = iota((seqs, seqs), 0) == iota((seqs, seqs), 1)
    len_col = jnp.sum(jnp.where(eye, len_row, 0.0), axis=1, keepdims=True)
    lane1 = iota((1, lanes), 1)
    inv_lane = jnp.exp(mod(lane1, half).astype(F32) * (-math.log(ROPE_BASE) / half))
    ang = len_col * inv_lane
    cos_q, sin_q = jnp.cos(ang), jnp.sin(ang)

    width = heads * qk
    src_i, out_c = iota((width, lanes), 0), iota((width, lanes), 1)
    pick_n = jnp.where(src_i == div(out_c, NOPE) * qk + mod(out_c, NOPE), 1.0, 0.0).astype(BF)
    rope_head, rope_p = div(out_c, ropes), mod(out_c, ropes)
    live = out_c < heads * ropes
    pick_a = jnp.where(live & (src_i == rope_head * qk + NOPE + rope_p), 1.0, 0.0)
    pick_b = jnp.where(
        live & (src_i == rope_head * qk + NOPE + mod(rope_p + half, ropes)),
        jnp.where(rope_p < half, -1.0, 1.0),
        0.0,
    )
    key_i, key_c = iota((ropes, lanes), 0), iota((ropes, lanes), 1)
    key_p = mod(key_c, ropes)
    key_a = jnp.where(key_i == key_p, 1.0, 0.0).astype(BF)
    key_b = jnp.where(key_i == mod(key_p + half, ropes), jnp.where(key_p < half, -1.0, 1.0), 0.0).astype(BF)
    key_new = (mm(new_rope, key_a) * cos_q + mm(new_rope, key_b) * sin_q).astype(BF)

    g_i, g_c = iota((qk, width), 0), iota((qk, width), 1)
    tile = jnp.zeros((qk, width), F32)
    for h in range(heads):
        tile = jnp.where(g_c - h * qk == g_i, 1.0, tile)
    loads[8].wait()
    gains = exact(query_gain[...], tile)
    lane_w = iota((1, width), 1)
    gain = gains[0:1]
    for h in range(1, heads):
        gain = jnp.where(lane_w >= h * qk, gains[h : h + 1], gain)

    row_i, seq_c = iota((rows, seqs), 0), iota((rows, seqs), 1)
    spread = jnp.where(div(row_i, block) * s_here + mod(row_i, s_here) == seq_c, 1.0, 0.0).astype(BF)
    mine_mask = me * s_here + mod(row_i, s_here) == seq_c
    mine = jnp.where(mine_mask, 1.0, 0.0).astype(BF)
    len_rows = jnp.sum(jnp.where(mine_mask, len_row, 0.0), axis=1, keepdims=True)
    row_l, lane_l = iota((rows, lanes), 0), iota((rows, lanes), 1)
    row_head = mod(div(row_l, s_here), heads)
    head_lanes = div(lane_l, NOPE) == row_head
    rope_lanes = div(lane_l, ropes) == row_head

    loads[13].wait()
    positions = crope.shape[2]
    inv_sub = jnp.exp(iota((half, positions), 0).astype(F32) * (-math.log(ROPE_BASE) / half))
    kang = inv_sub * iota((half, positions), 1).astype(F32)
    kcos, ksin = jnp.cos(kang), jnp.sin(kang)
    rotated = []
    pad = jnp.zeros((lanes - heads * ropes, positions), BF)
    for s in range(s_here):
        u = crope[s, :half, :].astype(F32)
        w = crope[s, half:, :].astype(F32)
        a = (u * kcos - w * ksin).astype(BF)
        b = (w * kcos + u * ksin).astype(BF)
        rotated.append(jnp.concatenate([a, b] * heads + [pad], axis=0))

    arrive(0, own_lat, lat_at)
    q_raw = jnp.concatenate([lat_buf[t, :, :qc] for t in range(tp_n)], axis=1).astype(F32)
    kv_raw = jnp.concatenate([lat_buf[t, :, qc:] for t in range(tp_n)], axis=1).astype(F32)
    loads[5].wait()
    q_lat = (q_raw * lax.rsqrt(jnp.mean(q_raw * q_raw, axis=-1, keepdims=True) + EPS) * q_gain[...]).astype(BF)
    loads[7].wait()
    query = mm_nt(q_lat, q_up[...])
    scale = jnp.zeros_like(query)
    lane_q = iota(query.shape, 1)
    for h in range(heads):
        inside = (lane_q >= h * qk) & (lane_q < (h + 1) * qk)
        total = jnp.sum(jnp.where(inside, query * query, 0.0), axis=-1, keepdims=True)
        scale = jnp.where(inside, lax.rsqrt(total * (1.0 / qk) + EPS), scale)
    query = query * scale * gain
    nope = mm(query.astype(BF), pick_n).astype(BF)
    rot = (exact(query, pick_a) * cos_q + exact(query, pick_b) * sin_q).astype(BF)
    nope_rows = jnp.where(head_lanes, mm(spread, nope), 0.0).astype(BF)
    rot_rows = jnp.where(rope_lanes, mm(spread, rot), 0.0).astype(BF)
    loads[9].wait()
    absorbed = mm_nt(nope_rows, key_up[...]).astype(BF)
    for t in range(tp_n):
        query_out[t, :, :rank] = absorbed[t * block : (t + 1) * block]
        query_out[t, :, rank:] = rot_rows[t * block : (t + 1) * block]
    q_src = lambda to: query_out.at[to]
    q_dst = lambda i: query_in.at[i]
    exchange(1, q_src, q_dst)
    query_in[me] = query_out[me]

    kv_scale = lax.rsqrt(jnp.mean(kv_raw * kv_raw, axis=-1, keepdims=True) + EPS)
    loads[6].wait()
    latent_new = (kv_raw * kv_scale * kv_gain[...]).astype(BF)
    own_cols = pl.ds(pl.multiple_of(me * kc, kc), kc)
    latent_ref[...] = (kv_part.astype(F32) * kv_scale * kv_gain[:, own_cols]).astype(BF)
    latent_rows = mm(mine, latent_new)
    key_rows = mm(mine, key_new)
    loads[12].wait()

    arrive(1, q_src, q_dst)
    q_abs = jnp.concatenate([query_in[t, :, :rank] for t in range(tp_n)], axis=0)
    q_rot = jnp.concatenate([query_in[t, :, rank:] for t in range(tp_n)], axis=0)
    row_p, pos_p = iota((rows, positions), 0), iota((rows, positions), 1)
    row_seq = mod(row_p, s_here)
    scores = jnp.zeros((rows, positions), F32)
    for s in range(s_here):
        scores = jnp.where(row_seq == s, mm_nt(q_abs, cache[s]) + mm(q_rot, rotated[s]), scores)
    score_scale = qk ** (-0.5)
    scores = scores * score_scale
    self_score = (
        jnp.sum(q_abs.astype(F32) * latent_rows, axis=-1, keepdims=True)
        + jnp.sum(q_rot.astype(F32) * key_rows, axis=-1, keepdims=True)
    ) * score_scale
    valid = pos_p.astype(F32) < len_rows
    scores = jnp.where(valid, scores, -jnp.inf)
    top = jnp.maximum(jnp.max(scores, axis=-1, keepdims=True), self_score)
    weights = jnp.exp(scores - top)
    self_weight = jnp.exp(self_score - top)
    total = jnp.sum(weights, axis=-1, keepdims=True) + self_weight
    acc = self_weight.astype(BF).astype(F32) * latent_rows
    for s in range(s_here):
        acc = acc + mm(jnp.where(row_seq == s, weights, 0.0).astype(BF), cache[s])
    attended = (acc / total).astype(BF)
    for t in range(tp_n):
        att_out[t] = attended[t * block : (t + 1) * block]
    a_src = lambda to: att_out.at[to]
    a_dst = lambda i: att_in.at[i]
    exchange(2, a_src, a_dst)
    att_in[me] = att_out[me]
    loads[10].wait()
    loads[11].wait()
    seq_i, row_c = iota((seqs, rows), 0), iota((seqs, rows), 1)
    gather = jnp.where(div(row_c, block) * s_here + mod(row_c, s_here) == seq_i, 1.0, 0.0).astype(BF)

    arrive(2, a_src, a_dst)
    att = jnp.concatenate([att_in[t] for t in range(tp_n)], axis=0)
    values = jnp.where(head_lanes, mm(att, value_up[...]), 0.0).astype(BF)
    head_values = mm(gather, values).astype(BF)
    partial = mm(head_values, attn_out[...]).astype(BF)
    for t in range(tp_n):
        sum_out[t] = partial[:, t * cols : (t + 1) * cols]
    s_src = lambda to: sum_out.at[to]
    s_dst = lambda i: sum_in.at[i]
    exchange(3, s_src, s_dst)
    sum_in[me] = sum_out[me]
    model_cols = pl.ds(pl.multiple_of(me * cols, cols), cols)
    tok_mine = tokens[:, model_cols].astype(F32)
    for i in (15, 16, 17, 18, 19, 20):
        loads[i].wait()
    eye_row = lambda row: jnp.sum(jnp.where(eye, row, 0.0), axis=1, keepdims=True)
    topk = route.shape[0]
    chosen = [eye_row(route[k : k + 1, :].astype(F32)) for k in range(topk)]
    chosen_weight = [eye_row(route_weight[k : k + 1, :]) for k in range(topk)]

    arrive(3, s_src, s_dst)
    head_sum = sum_in[0].astype(F32)
    for t in range(1, tp_n):
        head_sum = head_sum + sum_in[t].astype(F32)
    resid = (tok_mine + head_sum).astype(BF)
    rows_in[me, ep_me] = resid

    def rows_copy(origin, to):
        return pltpu.make_async_remote_copy(
            src_ref=rows_in.at[me, origin],
            dst_ref=rows_in.at[me, origin],
            send_sem=bulk.at[0],
            recv_sem=rows_recv.at[origin],
            device_id=(to, me),
            device_id_type=MESH,
        )

    def pass_on(origin):
        for k in range(1, tp_n):
            pltpu.make_async_remote_copy(
                src_ref=rows_in.at[me, origin],
                dst_ref=rows_in.at[me, origin],
                send_sem=bulk.at[1],
                recv_sem=bulk.at[2],
                device_id=(ep_me, lax.rem(me + k, tp_n)),
                device_id_type=MESH,
            ).start()

    def by_distance(k):
        away = lax.div(k + 1, 2)
        return lax.rem(jnp.where(lax.rem(k, 2) == 1, ep_me + away, ep_me + ep_n - away), ep_n)

    def give_rows(k, carry):
        rows_copy(ep_me, by_distance(ep_n - k)).start()
        return carry

    lax.fori_loop(1, ep_n, give_rows, 0)
    pass_on(ep_me)

    def take_rows(k, carry):
        origin = by_distance(k)
        rows_copy(origin, origin).wait_recv()
        pass_on(origin)
        return carry

    lax.fori_loop(1, ep_n, take_rows, 0)

    def bulk_wait(ref, sem):
        return pltpu.make_async_copy(ref, ref, sem)

    most = rows_in.at[pl.ds(0, tp_n - 1)]
    bulk_wait(most, bulk.at[2]).wait()

    group = math.gcd(ep_n, 8)

    def expert(g, carry):
        first = g * group
        parts = []
        square = jnp.zeros((group * seqs, 1), F32)
        for t in range(tp_n):
            x = jnp.concatenate([rows_in[t, first + i] for i in range(group)], axis=0).astype(F32)
            square = square + jnp.sum(x * x, axis=-1, keepdims=True)
            parts.append(x)
        inverse = lax.rsqrt(square * (1.0 / (cols * tp_n)) + EPS)
        gate = jnp.zeros((group * seqs, gate_w.shape[2]), F32)
        up = jnp.zeros((group * seqs, gate_w.shape[2]), F32)
        for t in range(tp_n):
            here = slice(t * cols, (t + 1) * cols)
            x = (parts[t] * inverse * moe_gain[:, here]).astype(BF)
            gate = gate + mm(x, gate_w[0, here, :])
            up = up + mm(x, up_w[0, here, :])
        hidden = (gate / (1.0 + jnp.exp(-gate)) * up).astype(BF)
        for t in range(tp_n):
            here = slice(t * cols, (t + 1) * cols)
            part = mm(hidden, down_w[0, :, here]).astype(BF)
            for i in range(group):
                part_out[t, first + i] = part[i * seqs : (i + 1) * seqs]
        return carry

    if ep_n == group:
        expert(0, 0)
    else:
        lax.fori_loop(0, ep_n // group, expert, 0)

    def part_copy(to_tp, block_ep, origin):
        return pltpu.make_async_remote_copy(
            src_ref=part_out.at[to_tp, block_ep],
            dst_ref=part_in.at[origin, block_ep],
            send_sem=bulk.at[3],
            recv_sem=part_recv.at[block_ep, origin],
            device_id=(ep_me, to_tp),
            device_id_type=MESH,
        )

    def give_parts(k, carry):
        block_ep = by_distance(ep_n - k)
        for j in range(1, tp_n):
            part_copy(lax.rem(me + j, tp_n), block_ep, me).start()
        return carry

    lax.fori_loop(1, ep_n + 1, give_parts, 0)

    def back_copy(to):
        return pltpu.make_async_remote_copy(
            src_ref=back_out.at[to],
            dst_ref=back_in.at[ep_me],
            send_sem=bulk.at[4],
            recv_sem=bulk.at[5],
            device_id=(to, me),
            device_id_type=MESH,
        )

    def summed(block_ep):
        found = part_out[me, block_ep].astype(F32)
        for j in range(1, tp_n):
            origin = lax.rem(me + j, tp_n)
            part_copy(origin, block_ep, origin).wait_recv()
            found = found + part_in[origin, block_ep].astype(F32)
        return found.astype(BF)

    def give_back(k, carry):
        to = by_distance(ep_n - k)
        back_out[to] = summed(to)
        back_copy(to).start()
        return carry

    lax.fori_loop(1, ep_n, give_back, 0)
    back_in[ep_me] = summed(ep_me)

    def share_of(e):
        share = jnp.zeros((seqs, 1), F32)
        for k in range(topk):
            share = share + jnp.where(chosen[k] == jnp.float32(e), chosen_weight[k], 0.0)
        return share

    few = ep_n <= 8
    shares = [share_of(e) for e in range(ep_n)] if few else None
    bulk_wait(back_in.at[pl.ds(0, ep_n - 1)], bulk.at[5]).wait()
    mixed = jnp.zeros((seqs, cols), F32)
    if few:
        for e in range(ep_n):
            mixed = mixed + shares[e] * back_in[e].astype(F32)
    else:
        mixed = lax.fori_loop(
            0, ep_n, lambda e, m: m + share_of(lax.convert_element_type(e, F32)) * back_in[e].astype(F32), mixed
        )
    mixed_ref[...] = (resid.astype(F32) + mixed).astype(BF)

    sent(0, own_lat, lat_at)
    sent(1, q_src, q_dst)
    sent(2, a_src, a_dst)
    sent(3, s_src, s_dst)
    bulk_wait(back_out.at[pl.ds(0, ep_n - 1)], bulk.at[0]).wait()
    bulk_wait(most, bulk.at[1]).wait()
    bulk_wait(most, bulk.at[3]).wait()
    bulk_wait(back_out.at[pl.ds(0, ep_n - 1)], bulk.at[4]).wait()


def finish(a, b, c, x, y, z):
    x[...] = a[...]
    y[...] = b[...]
    z[...] = c[...]


def shards(ep_n, tp_n, *args):
    (
        tokens,
        attn_gain,
        q_down,
        kv_down,
        rope_down,
        q_latent_gain,
        kv_latent_gain,
        q_up,
        query_gain,
        key_up,
        value_up,
        attn_out,
        cache_latent,
        cache_rope,
        lengths,
        moe_gain,
        route,
        route_weight,
        expert_gate,
        expert_up,
        expert_down,
    ) = args
    assert expert_gate.shape[0] == 1
    row = lambda v: v.reshape(1, -1)
    operands = (
        tokens,
        row(attn_gain),
        q_down,
        kv_down,
        rope_down.T,
        row(q_latent_gain),
        row(kv_latent_gain),
        q_up.T,
        query_gain,
        key_up,
        value_up,
        attn_out,
        cache_latent,
        cache_rope,
        row(lengths),
        row(moe_gain),
        route.T,
        route_weight.T,
        expert_gate,
        expert_up,
        expert_down,
    )
    vmem = pl.BlockSpec(memory_space=pltpu.VMEM)
    anyspace = pl.BlockSpec(memory_space=pltpu.HBM)
    seqs, model = tokens.shape
    cols = model // tp_n
    n = ep_n * tp_n
    heads = query_gain.shape[0]
    s_here, _, rank = cache_latent.shape
    block = heads * s_here
    like = lambda v: pltpu.VMEM(v.shape, v.dtype)
    scratch = [like(v) for v in operands] + [
        pltpu.VMEM((tp_n, seqs, q_down.shape[1] + kv_down.shape[1]), BF),
        pltpu.VMEM((tp_n, block, rank + 128), BF),
        pltpu.VMEM((tp_n, block, rank + 128), BF),
        pltpu.VMEM((tp_n, block, rank), BF),
        pltpu.VMEM((tp_n, block, rank), BF),
        pltpu.VMEM((tp_n, seqs, cols), BF),
        pltpu.VMEM((tp_n, seqs, cols), BF),
        pltpu.VMEM((tp_n, ep_n, seqs, cols), BF),
        pltpu.VMEM((tp_n, ep_n, seqs, cols), BF),
        pltpu.VMEM((tp_n, ep_n, seqs, cols), BF),
        pltpu.VMEM((ep_n, seqs, cols), BF),
        pltpu.VMEM((ep_n, seqs, cols), BF),
        pltpu.SemaphoreType.DMA((len(operands),)),
        pltpu.SemaphoreType.DMA((4, tp_n)),
        pltpu.SemaphoreType.DMA((4, tp_n)),
        pltpu.SemaphoreType.DMA((ep_n,)),
        pltpu.SemaphoreType.DMA((ep_n, tp_n)),
        pltpu.SemaphoreType.DMA((6,)),
    ]
    outs = (
        jax.ShapeDtypeStruct((seqs, cols), BF),
        jax.ShapeDtypeStruct((seqs, kv_down.shape[1]), BF),
        jax.ShapeDtypeStruct((seqs, rope_down.shape[1]), BF),
    )
    grant = 60 * 1024 * 1024
    found = pl.pallas_call(
        functools.partial(kernel, ep_n, tp_n, len(operands)),
        out_shape=outs,
        in_specs=[anyspace] * len(operands),
        out_specs=(vmem, vmem, vmem),
        scratch_shapes=scratch,
        compiler_params=pltpu.CompilerParams(collective_id=0, has_side_effects=True, vmem_limit_bytes=grant),
    )(*operands)
    return pl.pallas_call(finish, out_shape=outs, in_specs=[vmem] * 3, out_specs=(vmem, vmem, vmem), compiler_params=pltpu.CompilerParams(vmem_limit_bytes=1024 * 1024))(*found)


def solution(mesh):
    placed = (
        P("ep", None),
        P(),
        P(None, "tp"),
        P(None, "tp"),
        P(),
        P(),
        P(),
        P(None, "tp"),
        P("tp", None),
        P(None, "tp"),
        P(None, "tp"),
        P("tp", None),
        P(("ep", "tp"), None, None),
        P(("ep", "tp"), None, None),
        P("ep"),
        P(),
        P("ep", None),
        P("ep", None),
        P("ep", None, "tp"),
        P("ep", None, "tp"),
        P("ep", "tp", None),
    )
    return jax.shard_map(
        functools.partial(shards, mesh.shape["ep"], mesh.shape["tp"]),
        mesh=mesh,
        in_specs=placed,
        out_specs=(P("ep", "tp"), P("ep", "tp"), P("ep", None)),
        check_vma=False,
    )
```

```python
import functools
import math

import jax
import jax.numpy as jnp
from jax import lax
from jax.experimental import pallas as pl
from jax.experimental.pallas import tpu as pltpu
from jax.sharding import PartitionSpec as P

NOPE = 64
EPS = 1e-06
ROPE_BASE = 10000.0
MESH = pl.DeviceIdType.MESH
BF = jnp.bfloat16
F32 = jnp.float32


def shift_of(n):
    s = n.bit_length() - 1
    assert 1 << s == n
    return s


def div(v, n):
    return lax.shift_right_logical(v, jnp.int32(shift_of(n)))


def mod(v, n):
    return jnp.bitwise_and(v, jnp.int32(n - 1))


def iota(shape, dim):
    return lax.broadcasted_iota(jnp.int32, shape, dim)


def mm(a, b):
    return jnp.dot(a, b, preferred_element_type=F32)


def mm_nt(a, b):
    return lax.dot_general(a, b, (((1,), (1,)), ((), ())), preferred_element_type=F32)


def exact(a, b):
    return jnp.dot(a, b, preferred_element_type=F32, precision=lax.Precision.HIGHEST)


def kernel(ep_n, tp_n, count, *refs):
    far = refs[:count]
    mixed_ref, latent_ref, rope_ref = refs[count : count + 3]
    near = refs[count + 3 : 2 * count + 3]
    (
        tokens,
        attn_gain,
        q_down,
        kv_down,
        rope_down,
        q_gain,
        kv_gain,
        q_up,
        query_gain,
        key_up,
        value_up,
        attn_out,
        cache,
        crope,
        lengths,
        moe_gain,
        route,
        route_weight,
        gate_w,
        up_w,
        down_w,
    ) = near
    (
        lat_buf,
        query_out,
        query_in,
        att_out,
        att_in,
        sum_out,
        sum_in,
        rows_in,
        part_out,
        part_in,
        back_out,
        back_in,
        load_sem,
        tp_send,
        tp_recv,
        rows_recv,
        part_recv,
        bulk,
        near_sem,
    ) = refs[2 * count + 3 :]
    ep_me = lax.axis_index("ep")
    me = lax.axis_index("tp")
    seqs = tokens.shape[0]
    cols = tokens.shape[1] // tp_n
    heads, qk = query_gain.shape
    ropes = qk - NOPE
    half = ropes // 2
    s_here = cache.shape[0]
    rank = cache.shape[2]
    rows = tp_n * heads * s_here
    block = heads * s_here
    lanes = 128

    loads = [pltpu.make_async_copy(far[i], near[i], load_sem.at[i]) for i in range(count)]
    for i in (0, 1, 2, 3, 4, 14, 5, 6, 7, 8, 9, 13, 12, 10, 11, 15, 16, 17, 18, 19, 20):
        loads[i].start()

    barrier = pltpu.get_barrier_semaphore()
    for k in range(1, tp_n):
        pl.semaphore_signal(barrier, inc=1, device_id=(ep_me, lax.rem(me + k, tp_n)), device_id_type=MESH)

    pair, pairs = ep_me // 2, ep_n // 2
    sides = (
        (pair >= 0, ep_me + 1 - 2 * lax.rem(ep_me, 2), 0),
        (pair > 0, ep_me - 2, 2),
        (pair < pairs - 1, ep_me + 2, 1),
    )

    def each_side(act):
        for slot, (there, peer, seen) in enumerate(sides):

            @pl.when(there)
            def _():
                act(slot, peer, seen)

    each_side(
        lambda slot, peer, seen: pl.semaphore_signal(
            barrier, inc=1, device_id=(peer, me), device_id_type=MESH
        )
    )

    def tell():
        each_side(
            lambda slot, peer, seen: pl.semaphore_signal(
                near_sem.at[seen], inc=1, device_id=(peer, me), device_id_type=MESH
            )
        )

    def hear():
        each_side(lambda slot, peer, seen: pl.semaphore_wait(near_sem.at[slot], 1))

    def tp_copy(stage, src, dst, to, origin):
        return pltpu.make_async_remote_copy(
            src_ref=src,
            dst_ref=dst,
            send_sem=tp_send.at[stage, to],
            recv_sem=tp_recv.at[stage, origin],
            device_id=(ep_me, to),
            device_id_type=MESH,
        )

    def exchange(stage, src_of, dst_of):
        for k in range(1, tp_n):
            to = lax.rem(me + k, tp_n)
            tp_copy(stage, src_of(to), dst_of(me), to, me).start()

    def arrive(stage, src_of, dst_of):
        for k in range(1, tp_n):
            other = lax.rem(me + k, tp_n)
            tp_copy(stage, src_of(other), dst_of(other), other, other).wait_recv()

    def sent(stage, src_of, dst_of):
        for k in range(1, tp_n):
            other = lax.rem(me + k, tp_n)
            tp_copy(stage, src_of(other), dst_of(other), other, other).wait_send()

    loads[0].wait()
    loads[1].wait()
    tok = tokens[...].astype(F32)
    normed = (tok * lax.rsqrt(jnp.mean(tok * tok, axis=-1, keepdims=True) + EPS) * attn_gain[...]).astype(BF)
    loads[2].wait()
    qc = q_down.shape[1]
    kc = kv_down.shape[1]
    q_part = mm(normed, q_down[...]).astype(BF)
    loads[3].wait()
    kv_part = mm(normed, kv_down[...]).astype(BF)
    lat_buf[me, :, :qc] = q_part
    lat_buf[me, :, qc:] = kv_part
    pl.semaphore_wait(barrier, tp_n + jnp.where(pair > 0, 1, 0) + jnp.where(pair < pairs - 1, 1, 0))
    own_lat = lambda to: lat_buf.at[me]
    lat_at = lambda i: lat_buf.at[i]
    exchange(0, own_lat, lat_at)
    if pairs > 1:
        tell()

    loads[4].wait()
    loads[14].wait()
    new_rope = mm_nt(normed, rope_down[...]).astype(BF)
    rope_ref[...] = new_rope
    len_row = lengths[...].astype(F32)
    eye = iota((seqs, seqs), 0) == iota((seqs, seqs), 1)
    len_col = jnp.sum(jnp.where(eye, len_row, 0.0), axis=1, keepdims=True)
    lane1 = iota((1, lanes), 1)
    inv_lane = jnp.exp(mod(lane1, half).astype(F32) * (-math.log(ROPE_BASE) / half))
    ang = len_col * inv_lane
    cos_q, sin_q = jnp.cos(ang), jnp.sin(ang)

    width = heads * qk
    src_i, out_c = iota((width, lanes), 0), iota((width, lanes), 1)
    pick_n = jnp.where(src_i == div(out_c, NOPE) * qk + mod(out_c, NOPE), 1.0, 0.0).astype(BF)
    rope_head, rope_p = div(out_c, ropes), mod(out_c, ropes)
    live = out_c < heads * ropes
    pick_a = jnp.where(live & (src_i == rope_head * qk + NOPE + rope_p), 1.0, 0.0)
    pick_b = jnp.where(
        live & (src_i == rope_head * qk + NOPE + mod(rope_p + half, ropes)),
        jnp.where(rope_p < half, -1.0, 1.0),
        0.0,
    )
    key_i, key_c = iota((ropes, lanes), 0), iota((ropes, lanes), 1)
    key_p = mod(key_c, ropes)
    key_a = jnp.where(key_i == key_p, 1.0, 0.0).astype(BF)
    key_b = jnp.where(key_i == mod(key_p + half, ropes), jnp.where(key_p < half, -1.0, 1.0), 0.0).astype(BF)
    key_new = (mm(new_rope, key_a) * cos_q + mm(new_rope, key_b) * sin_q).astype(BF)

    g_i, g_c = iota((qk, width), 0), iota((qk, width), 1)
    tile = jnp.zeros((qk, width), F32)
    for h in range(heads):
        tile = jnp.where(g_c - h * qk == g_i, 1.0, tile)
    loads[8].wait()
    gains = exact(query_gain[...], tile)
    lane_w = iota((1, width), 1)
    gain = gains[0:1]
    for h in range(1, heads):
        gain = jnp.where(lane_w >= h * qk, gains[h : h + 1], gain)

    row_i, seq_c = iota((rows, seqs), 0), iota((rows, seqs), 1)
    spread = jnp.where(div(row_i, block) * s_here + mod(row_i, s_here) == seq_c, 1.0, 0.0).astype(BF)
    mine_mask = me * s_here + mod(row_i, s_here) == seq_c
    mine = jnp.where(mine_mask, 1.0, 0.0).astype(BF)
    len_rows = jnp.sum(jnp.where(mine_mask, len_row, 0.0), axis=1, keepdims=True)
    row_l, lane_l = iota((rows, lanes), 0), iota((rows, lanes), 1)
    row_head = mod(div(row_l, s_here), heads)
    head_lanes = div(lane_l, NOPE) == row_head
    rope_lanes = div(lane_l, ropes) == row_head

    loads[13].wait()
    positions = crope.shape[2]
    inv_sub = jnp.exp(iota((half, positions), 0).astype(F32) * (-math.log(ROPE_BASE) / half))
    kang = inv_sub * iota((half, positions), 1).astype(F32)
    kcos, ksin = jnp.cos(kang), jnp.sin(kang)
    rotated = []
    pad = jnp.zeros((lanes - heads * ropes, positions), BF)
    for s in range(s_here):
        u = crope[s, :half, :].astype(F32)
        w = crope[s, half:, :].astype(F32)
        a = (u * kcos - w * ksin).astype(BF)
        b = (w * kcos + u * ksin).astype(BF)
        rotated.append(jnp.concatenate([a, b] * heads + [pad], axis=0))

    arrive(0, own_lat, lat_at)
    q_raw = jnp.concatenate([lat_buf[t, :, :qc] for t in range(tp_n)], axis=1).astype(F32)
    kv_raw = jnp.concatenate([lat_buf[t, :, qc:] for t in range(tp_n)], axis=1).astype(F32)
    loads[5].wait()
    q_lat = (q_raw * lax.rsqrt(jnp.mean(q_raw * q_raw, axis=-1, keepdims=True) + EPS) * q_gain[...]).astype(BF)
    loads[7].wait()
    query = mm_nt(q_lat, q_up[...])
    scale = jnp.zeros_like(query)
    lane_q = iota(query.shape, 1)
    for h in range(heads):
        inside = (lane_q >= h * qk) & (lane_q < (h + 1) * qk)
        total = jnp.sum(jnp.where(inside, query * query, 0.0), axis=-1, keepdims=True)
        scale = jnp.where(inside, lax.rsqrt(total * (1.0 / qk) + EPS), scale)
    query = query * scale * gain
    nope = mm(query.astype(BF), pick_n).astype(BF)
    rot = (exact(query, pick_a) * cos_q + exact(query, pick_b) * sin_q).astype(BF)
    nope_rows = jnp.where(head_lanes, mm(spread, nope), 0.0).astype(BF)
    rot_rows = jnp.where(rope_lanes, mm(spread, rot), 0.0).astype(BF)
    loads[9].wait()
    absorbed = mm_nt(nope_rows, key_up[...]).astype(BF)
    for t in range(tp_n):
        query_out[t, :, :rank] = absorbed[t * block : (t + 1) * block]
        query_out[t, :, rank:] = rot_rows[t * block : (t + 1) * block]
    q_src = lambda to: query_out.at[to]
    q_dst = lambda i: query_in.at[i]
    exchange(1, q_src, q_dst)
    query_in[me] = query_out[me]
    if pairs > 2:
        hear()
        tell()

    kv_scale = lax.rsqrt(jnp.mean(kv_raw * kv_raw, axis=-1, keepdims=True) + EPS)
    loads[6].wait()
    latent_new = (kv_raw * kv_scale * kv_gain[...]).astype(BF)
    own_cols = pl.ds(pl.multiple_of(me * kc, kc), kc)
    latent_ref[...] = (kv_part.astype(F32) * kv_scale * kv_gain[:, own_cols]).astype(BF)
    latent_rows = mm(mine, latent_new)
    key_rows = mm(mine, key_new)
    loads[12].wait()

    arrive(1, q_src, q_dst)
    q_abs = jnp.concatenate([query_in[t, :, :rank] for t in range(tp_n)], axis=0)
    q_rot = jnp.concatenate([query_in[t, :, rank:] for t in range(tp_n)], axis=0)
    row_p, pos_p = iota((rows, positions), 0), iota((rows, positions), 1)
    row_seq = mod(row_p, s_here)
    scores = jnp.zeros((rows, positions), F32)
    for s in range(s_here):
        scores = jnp.where(row_seq == s, mm_nt(q_abs, cache[s]) + mm(q_rot, rotated[s]), scores)
    score_scale = qk ** (-0.5)
    scores = scores * score_scale
    self_score = (
        jnp.sum(q_abs.astype(F32) * latent_rows, axis=-1, keepdims=True)
        + jnp.sum(q_rot.astype(F32) * key_rows, axis=-1, keepdims=True)
    ) * score_scale
    valid = pos_p.astype(F32) < len_rows
    scores = jnp.where(valid, scores, -jnp.inf)
    top = jnp.maximum(jnp.max(scores, axis=-1, keepdims=True), self_score)
    weights = jnp.exp(scores - top)
    self_weight = jnp.exp(self_score - top)
    total = jnp.sum(weights, axis=-1, keepdims=True) + self_weight
    acc = self_weight.astype(BF).astype(F32) * latent_rows
    for s in range(s_here):
        acc = acc + mm(jnp.where(row_seq == s, weights, 0.0).astype(BF), cache[s])
    attended = (acc / total).astype(BF)
    for t in range(tp_n):
        att_out[t] = attended[t * block : (t + 1) * block]
    a_src = lambda to: att_out.at[to]
    a_dst = lambda i: att_in.at[i]
    exchange(2, a_src, a_dst)
    att_in[me] = att_out[me]

    def next_round(k, carry):
        hear()
        tell()
        return carry

    lax.fori_loop(2, pairs - 1, next_round, 0)
    loads[10].wait()
    loads[11].wait()
    seq_i, row_c = iota((seqs, rows), 0), iota((seqs, rows), 1)
    gather = jnp.where(div(row_c, block) * s_here + mod(row_c, s_here) == seq_i, 1.0, 0.0).astype(BF)

    arrive(2, a_src, a_dst)
    att = jnp.concatenate([att_in[t] for t in range(tp_n)], axis=0)
    values = jnp.where(head_lanes, mm(att, value_up[...]), 0.0).astype(BF)
    head_values = mm(gather, values).astype(BF)
    partial = mm(head_values, attn_out[...]).astype(BF)
    for t in range(tp_n):
        sum_out[t] = partial[:, t * cols : (t + 1) * cols]
    s_src = lambda to: sum_out.at[to]
    s_dst = lambda i: sum_in.at[i]
    exchange(3, s_src, s_dst)
    sum_in[me] = sum_out[me]
    if pairs > 1:
        hear()
    model_cols = pl.ds(pl.multiple_of(me * cols, cols), cols)
    tok_mine = tokens[:, model_cols].astype(F32)
    for i in (15, 16, 17, 18, 19, 20):
        loads[i].wait()
    eye_row = lambda row: jnp.sum(jnp.where(eye, row, 0.0), axis=1, keepdims=True)
    topk = route.shape[0]
    chosen = [eye_row(route[k : k + 1, :].astype(F32)) for k in range(topk)]
    chosen_weight = [eye_row(route_weight[k : k + 1, :]) for k in range(topk)]

    arrive(3, s_src, s_dst)
    head_sum = sum_in[0].astype(F32)
    for t in range(1, tp_n):
        head_sum = head_sum + sum_in[t].astype(F32)
    resid = (tok_mine + head_sum).astype(BF)
    rows_in[me, ep_me] = resid

    def rows_copy(origin, to):
        return pltpu.make_async_remote_copy(
            src_ref=rows_in.at[me, origin],
            dst_ref=rows_in.at[me, origin],
            send_sem=bulk.at[0],
            recv_sem=rows_recv.at[origin],
            device_id=(to, me),
            device_id_type=MESH,
        )

    def pass_on(origin):
        for k in range(1, tp_n):
            pltpu.make_async_remote_copy(
                src_ref=rows_in.at[me, origin],
                dst_ref=rows_in.at[me, origin],
                send_sem=bulk.at[1],
                recv_sem=bulk.at[2],
                device_id=(ep_me, lax.rem(me + k, tp_n)),
                device_id_type=MESH,
            ).start()

    def at_distance(d, act):
        @pl.when(ep_me + d < ep_n)
        def _():
            act(ep_me + d)

        @pl.when(ep_me >= d)
        def _():
            act(ep_me - d)

    def farthest_first(act):
        def step(k, carry):
            at_distance(ep_n - k, act)
            return carry

        lax.fori_loop(1, ep_n, step, 0)

    def nearest_first(act):
        def step(k, carry):
            at_distance(k, act)
            return carry

        lax.fori_loop(1, ep_n, step, 0)

    farthest_first(lambda to: rows_copy(ep_me, to).start())
    pass_on(ep_me)

    def take_rows(origin):
        rows_copy(origin, origin).wait_recv()
        pass_on(origin)

    nearest_first(take_rows)

    def bulk_wait(ref, sem):
        return pltpu.make_async_copy(ref, ref, sem)

    most = rows_in.at[pl.ds(0, tp_n - 1)]
    bulk_wait(most, bulk.at[2]).wait()

    group = math.gcd(ep_n, 8)

    def expert(g, carry):
        first = g * group
        parts = []
        square = jnp.zeros((group * seqs, 1), F32)
        for t in range(tp_n):
            x = jnp.concatenate([rows_in[t, first + i] for i in range(group)], axis=0).astype(F32)
            square = square + jnp.sum(x * x, axis=-1, keepdims=True)
            parts.append(x)
        inverse = lax.rsqrt(square * (1.0 / (cols * tp_n)) + EPS)
        gate = jnp.zeros((group * seqs, gate_w.shape[2]), F32)
        up = jnp.zeros((group * seqs, gate_w.shape[2]), F32)
        for t in range(tp_n):
            here = slice(t * cols, (t + 1) * cols)
            x = (parts[t] * inverse * moe_gain[:, here]).astype(BF)
            gate = gate + mm(x, gate_w[0, here, :])
            up = up + mm(x, up_w[0, here, :])
        hidden = (gate / (1.0 + jnp.exp(-gate)) * up).astype(BF)
        for t in range(tp_n):
            here = slice(t * cols, (t + 1) * cols)
            part = mm(hidden, down_w[0, :, here]).astype(BF)
            for i in range(group):
                part_out[t, first + i] = part[i * seqs : (i + 1) * seqs]
        return carry

    if ep_n == group:
        expert(0, 0)
    else:
        lax.fori_loop(0, ep_n // group, expert, 0)

    def part_copy(to_tp, block_ep, origin):
        return pltpu.make_async_remote_copy(
            src_ref=part_out.at[to_tp, block_ep],
            dst_ref=part_in.at[origin, block_ep],
            send_sem=bulk.at[3],
            recv_sem=part_recv.at[block_ep, origin],
            device_id=(ep_me, to_tp),
            device_id_type=MESH,
        )

    def give_parts(block_ep):
        for j in range(1, tp_n):
            part_copy(lax.rem(me + j, tp_n), block_ep, me).start()

    farthest_first(give_parts)
    give_parts(ep_me)

    def back_copy(to):
        return pltpu.make_async_remote_copy(
            src_ref=back_out.at[to],
            dst_ref=back_in.at[ep_me],
            send_sem=bulk.at[4],
            recv_sem=bulk.at[5],
            device_id=(to, me),
            device_id_type=MESH,
        )

    def summed(block_ep):
        found = part_out[me, block_ep].astype(F32)
        for j in range(1, tp_n):
            origin = lax.rem(me + j, tp_n)
            part_copy(origin, block_ep, origin).wait_recv()
            found = found + part_in[origin, block_ep].astype(F32)
        return found.astype(BF)

    def give_back(to):
        back_out[to] = summed(to)
        back_copy(to).start()

    farthest_first(give_back)
    back_in[ep_me] = summed(ep_me)

    def share_of(e):
        share = jnp.zeros((seqs, 1), F32)
        for k in range(topk):
            share = share + jnp.where(chosen[k] == jnp.float32(e), chosen_weight[k], 0.0)
        return share

    few = ep_n <= 8
    shares = [share_of(e) for e in range(ep_n)] if few else None
    bulk_wait(back_in.at[pl.ds(0, ep_n - 1)], bulk.at[5]).wait()
    mixed = jnp.zeros((seqs, cols), F32)
    if few:
        for e in range(ep_n):
            mixed = mixed + shares[e] * back_in[e].astype(F32)
    else:
        mixed = lax.fori_loop(
            0, ep_n, lambda e, m: m + share_of(lax.convert_element_type(e, F32)) * back_in[e].astype(F32), mixed
        )
    mixed_ref[...] = (resid.astype(F32) + mixed).astype(BF)

    sent(0, own_lat, lat_at)
    sent(1, q_src, q_dst)
    sent(2, a_src, a_dst)
    sent(3, s_src, s_dst)
    bulk_wait(back_out.at[pl.ds(0, ep_n - 1)], bulk.at[0]).wait()
    bulk_wait(most, bulk.at[1]).wait()
    bulk_wait(most, bulk.at[3]).wait()
    bulk_wait(back_out.at[pl.ds(0, ep_n - 1)], bulk.at[4]).wait()


def finish(a, b, c, x, y, z):
    x[...] = a[...]
    y[...] = b[...]
    z[...] = c[...]


def shards(ep_n, tp_n, *args):
    (
        tokens,
        attn_gain,
        q_down,
        kv_down,
        rope_down,
        q_latent_gain,
        kv_latent_gain,
        q_up,
        query_gain,
        key_up,
        value_up,
        attn_out,
        cache_latent,
        cache_rope,
        lengths,
        moe_gain,
        route,
        route_weight,
        expert_gate,
        expert_up,
        expert_down,
    ) = args
    assert expert_gate.shape[0] == 1 and ep_n % 2 == 0
    row = lambda v: v.reshape(1, -1)
    operands = (
        tokens,
        row(attn_gain),
        q_down,
        kv_down,
        rope_down.T,
        row(q_latent_gain),
        row(kv_latent_gain),
        q_up.T,
        query_gain,
        key_up,
        value_up,
        attn_out,
        cache_latent,
        cache_rope,
        row(lengths),
        row(moe_gain),
        route.T,
        route_weight.T,
        expert_gate,
        expert_up,
        expert_down,
    )
    vmem = pl.BlockSpec(memory_space=pltpu.VMEM)
    anyspace = pl.BlockSpec(memory_space=pltpu.HBM)
    seqs, model = tokens.shape
    cols = model // tp_n
    n = ep_n * tp_n
    heads = query_gain.shape[0]
    s_here, _, rank = cache_latent.shape
    block = heads * s_here
    like = lambda v: pltpu.VMEM(v.shape, v.dtype)
    scratch = [like(v) for v in operands] + [
        pltpu.VMEM((tp_n, seqs, q_down.shape[1] + kv_down.shape[1]), BF),
        pltpu.VMEM((tp_n, block, rank + 128), BF),
        pltpu.VMEM((tp_n, block, rank + 128), BF),
        pltpu.VMEM((tp_n, block, rank), BF),
        pltpu.VMEM((tp_n, block, rank), BF),
        pltpu.VMEM((tp_n, seqs, cols), BF),
        pltpu.VMEM((tp_n, seqs, cols), BF),
        pltpu.VMEM((tp_n, ep_n, seqs, cols), BF),
        pltpu.VMEM((tp_n, ep_n, seqs, cols), BF),
        pltpu.VMEM((tp_n, ep_n, seqs, cols), BF),
        pltpu.VMEM((ep_n, seqs, cols), BF),
        pltpu.VMEM((ep_n, seqs, cols), BF),
        pltpu.SemaphoreType.DMA((len(operands),)),
        pltpu.SemaphoreType.DMA((4, tp_n)),
        pltpu.SemaphoreType.DMA((4, tp_n)),
        pltpu.SemaphoreType.DMA((ep_n,)),
        pltpu.SemaphoreType.DMA((ep_n, tp_n)),
        pltpu.SemaphoreType.DMA((6,)),
        pltpu.SemaphoreType.REGULAR((3,)),
    ]
    outs = (
        jax.ShapeDtypeStruct((seqs, cols), BF),
        jax.ShapeDtypeStruct((seqs, kv_down.shape[1]), BF),
        jax.ShapeDtypeStruct((seqs, rope_down.shape[1]), BF),
    )
    grant = 60 * 1024 * 1024
    found = pl.pallas_call(
        functools.partial(kernel, ep_n, tp_n, len(operands)),
        out_shape=outs,
        in_specs=[anyspace] * len(operands),
        out_specs=(vmem, vmem, vmem),
        scratch_shapes=scratch,
        compiler_params=pltpu.CompilerParams(collective_id=0, has_side_effects=True, vmem_limit_bytes=grant),
    )(*operands)
    return pl.pallas_call(finish, out_shape=outs, in_specs=[vmem] * 3, out_specs=(vmem, vmem, vmem), compiler_params=pltpu.CompilerParams(vmem_limit_bytes=grant))(*found)


def solution(mesh):
    placed = (
        P("ep", None),
        P(),
        P(None, "tp"),
        P(None, "tp"),
        P(),
        P(),
        P(),
        P(None, "tp"),
        P("tp", None),
        P(None, "tp"),
        P(None, "tp"),
        P("tp", None),
        P(("ep", "tp"), None, None),
        P(("ep", "tp"), None, None),
        P("ep"),
        P(),
        P("ep", None),
        P("ep", None),
        P("ep", None, "tp"),
        P("ep", None, "tp"),
        P("ep", "tp", None),
    )
    return jax.shard_map(
        functools.partial(shards, mesh.shape["ep"], mesh.shape["tp"]),
        mesh=mesh,
        in_specs=placed,
        out_specs=(P("ep", "tp"), P("ep", "tp"), P("ep", None)),
        check_vma=False,
    )
```

```python
import functools
import math

import jax
import jax.numpy as jnp
from jax import lax
from jax.experimental import pallas as pl
from jax.experimental.pallas import tpu as pltpu
from jax.sharding import PartitionSpec as P

NOPE = 64
EPS = 1e-06
ROPE_BASE = 10000.0
MESH = pl.DeviceIdType.MESH
BF = jnp.bfloat16
F32 = jnp.float32


def shift_of(n):
    s = n.bit_length() - 1
    assert 1 << s == n
    return s


def div(v, n):
    return lax.shift_right_logical(v, jnp.int32(shift_of(n)))


def mod(v, n):
    return jnp.bitwise_and(v, jnp.int32(n - 1))


def iota(shape, dim):
    return lax.broadcasted_iota(jnp.int32, shape, dim)


def mm(a, b):
    return jnp.dot(a, b, preferred_element_type=F32)


def mm_nt(a, b):
    return lax.dot_general(a, b, (((1,), (1,)), ((), ())), preferred_element_type=F32)


def exact(a, b):
    return jnp.dot(a, b, preferred_element_type=F32, precision=lax.Precision.HIGHEST)


def kernel(ep_n, tp_n, count, *refs):
    far = refs[:count]
    mixed_ref, latent_ref, rope_ref = refs[count : count + 3]
    near = refs[count + 3 : 2 * count + 3]
    (
        tokens,
        attn_gain,
        q_down,
        kv_down,
        rope_down,
        q_gain,
        kv_gain,
        q_up,
        query_gain,
        key_up,
        value_up,
        attn_out,
        cache,
        crope,
        lengths,
        moe_gain,
        route,
        route_weight,
        gate_w,
        up_w,
        down_w,
    ) = near
    (
        lat_buf,
        query_out,
        query_in,
        att_out,
        att_in,
        sum_out,
        sum_in,
        rows_in,
        part_out,
        part_in,
        back_out,
        back_in,
        load_sem,
        tp_send,
        tp_recv,
        rows_recv,
        part_recv,
        bulk,
        near_sem,
    ) = refs[2 * count + 3 :]
    ep_me = lax.axis_index("ep")
    me = lax.axis_index("tp")
    seqs = tokens.shape[0]
    cols = tokens.shape[1] // tp_n
    heads, qk = query_gain.shape
    ropes = qk - NOPE
    half = ropes // 2
    s_here = cache.shape[0]
    rank = cache.shape[2]
    rows = tp_n * heads * s_here
    block = heads * s_here
    lanes = 128

    loads = [pltpu.make_async_copy(far[i], near[i], load_sem.at[i]) for i in range(count)]
    for i in (0, 1, 2, 3, 4, 14, 5, 6, 7, 8, 9, 13, 12, 10, 11, 15, 16, 17, 18, 19, 20):
        loads[i].start()

    barrier = pltpu.get_barrier_semaphore()
    for k in range(1, tp_n):
        pl.semaphore_signal(barrier, inc=1, device_id=(ep_me, lax.rem(me + k, tp_n)), device_id_type=MESH)

    pair, pairs = ep_me // 2, ep_n // 2
    sides = (
        (pair >= 0, ep_me + 1 - 2 * lax.rem(ep_me, 2), 0),
        (pair > 0, ep_me - 2, 2),
        (pair < pairs - 1, ep_me + 2, 1),
    )

    def each_side(act):
        for slot, (there, peer, seen) in enumerate(sides):

            @pl.when(there)
            def _():
                act(slot, peer, seen)

    each_side(
        lambda slot, peer, seen: pl.semaphore_signal(
            barrier, inc=1, device_id=(peer, me), device_id_type=MESH
        )
    )

    def tell():
        each_side(
            lambda slot, peer, seen: pl.semaphore_signal(
                near_sem.at[seen], inc=1, device_id=(peer, me), device_id_type=MESH
            )
        )

    def hear():
        each_side(lambda slot, peer, seen: pl.semaphore_wait(near_sem.at[slot], 1))

    def tp_copy(stage, src, dst, to, origin):
        return pltpu.make_async_remote_copy(
            src_ref=src,
            dst_ref=dst,
            send_sem=tp_send.at[stage, to],
            recv_sem=tp_recv.at[stage, origin],
            device_id=(ep_me, to),
            device_id_type=MESH,
        )

    def exchange(stage, src_of, dst_of):
        for k in range(1, tp_n):
            to = lax.rem(me + k, tp_n)
            tp_copy(stage, src_of(to), dst_of(me), to, me).start()

    def arrive(stage, src_of, dst_of):
        for k in range(1, tp_n):
            other = lax.rem(me + k, tp_n)
            tp_copy(stage, src_of(other), dst_of(other), other, other).wait_recv()

    def sent(stage, src_of, dst_of):
        for k in range(1, tp_n):
            other = lax.rem(me + k, tp_n)
            tp_copy(stage, src_of(other), dst_of(other), other, other).wait_send()

    loads[0].wait()
    loads[1].wait()
    tok = tokens[...].astype(F32)
    normed = (tok * lax.rsqrt(jnp.mean(tok * tok, axis=-1, keepdims=True) + EPS) * attn_gain[...]).astype(BF)
    loads[2].wait()
    qc = q_down.shape[1]
    kc = kv_down.shape[1]
    q_part = mm(normed, q_down[...]).astype(BF)
    loads[3].wait()
    kv_part = mm(normed, kv_down[...]).astype(BF)
    lat_buf[me, :, :qc] = q_part
    lat_buf[me, :, qc:] = kv_part
    pl.semaphore_wait(barrier, tp_n + jnp.where(pair > 0, 1, 0) + jnp.where(pair < pairs - 1, 1, 0))
    own_lat = lambda to: lat_buf.at[me]
    lat_at = lambda i: lat_buf.at[i]
    exchange(0, own_lat, lat_at)
    if pairs > 1:
        tell()

    loads[4].wait()
    loads[14].wait()
    new_rope = mm_nt(normed, rope_down[...]).astype(BF)
    rope_ref[...] = new_rope
    len_row = lengths[...].astype(F32)
    eye = iota((seqs, seqs), 0) == iota((seqs, seqs), 1)
    len_col = jnp.sum(jnp.where(eye, len_row, 0.0), axis=1, keepdims=True)
    lane1 = iota((1, lanes), 1)
    inv_lane = jnp.exp(mod(lane1, half).astype(F32) * (-math.log(ROPE_BASE) / half))
    ang = len_col * inv_lane
    cos_q, sin_q = jnp.cos(ang), jnp.sin(ang)

    width = heads * qk
    src_i, out_c = iota((width, lanes), 0), iota((width, lanes), 1)
    pick_n = jnp.where(src_i == div(out_c, NOPE) * qk + mod(out_c, NOPE), 1.0, 0.0).astype(BF)
    rope_head, rope_p = div(out_c, ropes), mod(out_c, ropes)
    live = out_c < heads * ropes
    pick_a = jnp.where(live & (src_i == rope_head * qk + NOPE + rope_p), 1.0, 0.0)
    pick_b = jnp.where(
        live & (src_i == rope_head * qk + NOPE + mod(rope_p + half, ropes)),
        jnp.where(rope_p < half, -1.0, 1.0),
        0.0,
    )
    key_i, key_c = iota((ropes, lanes), 0), iota((ropes, lanes), 1)
    key_p = mod(key_c, ropes)
    key_a = jnp.where(key_i == key_p, 1.0, 0.0).astype(BF)
    key_b = jnp.where(key_i == mod(key_p + half, ropes), jnp.where(key_p < half, -1.0, 1.0), 0.0).astype(BF)
    key_new = (mm(new_rope, key_a) * cos_q + mm(new_rope, key_b) * sin_q).astype(BF)

    g_i, g_c = iota((qk, width), 0), iota((qk, width), 1)
    tile = jnp.zeros((qk, width), F32)
    for h in range(heads):
        tile = jnp.where(g_c - h * qk == g_i, 1.0, tile)
    loads[8].wait()
    gains = exact(query_gain[...], tile)
    lane_w = iota((1, width), 1)
    gain = gains[0:1]
    for h in range(1, heads):
        gain = jnp.where(lane_w >= h * qk, gains[h : h + 1], gain)

    row_i, seq_c = iota((rows, seqs), 0), iota((rows, seqs), 1)
    spread = jnp.where(div(row_i, block) * s_here + mod(row_i, s_here) == seq_c, 1.0, 0.0).astype(BF)
    mine_mask = me * s_here + mod(row_i, s_here) == seq_c
    mine = jnp.where(mine_mask, 1.0, 0.0).astype(BF)
    len_rows = jnp.sum(jnp.where(mine_mask, len_row, 0.0), axis=1, keepdims=True)
    row_l, lane_l = iota((rows, lanes), 0), iota((rows, lanes), 1)
    row_head = mod(div(row_l, s_here), heads)
    head_lanes = div(lane_l, NOPE) == row_head
    rope_lanes = div(lane_l, ropes) == row_head

    loads[13].wait()
    positions = crope.shape[2]
    inv_sub = jnp.exp(iota((half, positions), 0).astype(F32) * (-math.log(ROPE_BASE) / half))
    kang = inv_sub * iota((half, positions), 1).astype(F32)
    kcos, ksin = jnp.cos(kang), jnp.sin(kang)
    rotated = []
    pad = jnp.zeros((lanes - heads * ropes, positions), BF)
    for s in range(s_here):
        u = crope[s, :half, :].astype(F32)
        w = crope[s, half:, :].astype(F32)
        a = (u * kcos - w * ksin).astype(BF)
        b = (w * kcos + u * ksin).astype(BF)
        rotated.append(jnp.concatenate([a, b] * heads + [pad], axis=0))

    arrive(0, own_lat, lat_at)
    q_raw = jnp.concatenate([lat_buf[t, :, :qc] for t in range(tp_n)], axis=1).astype(F32)
    kv_raw = jnp.concatenate([lat_buf[t, :, qc:] for t in range(tp_n)], axis=1).astype(F32)
    loads[5].wait()
    q_lat = (q_raw * lax.rsqrt(jnp.mean(q_raw * q_raw, axis=-1, keepdims=True) + EPS) * q_gain[...]).astype(BF)
    loads[7].wait()
    query = mm_nt(q_lat, q_up[...])
    scale = jnp.zeros_like(query)
    lane_q = iota(query.shape, 1)
    for h in range(heads):
        inside = (lane_q >= h * qk) & (lane_q < (h + 1) * qk)
        total = jnp.sum(jnp.where(inside, query * query, 0.0), axis=-1, keepdims=True)
        scale = jnp.where(inside, lax.rsqrt(total * (1.0 / qk) + EPS), scale)
    query = query * scale * gain
    nope = mm(query.astype(BF), pick_n).astype(BF)
    rot = (exact(query, pick_a) * cos_q + exact(query, pick_b) * sin_q).astype(BF)
    nope_rows = jnp.where(head_lanes, mm(spread, nope), 0.0).astype(BF)
    rot_rows = jnp.where(rope_lanes, mm(spread, rot), 0.0).astype(BF)
    loads[9].wait()
    absorbed = mm_nt(nope_rows, key_up[...]).astype(BF)
    for t in range(tp_n):
        query_out[t, :, :rank] = absorbed[t * block : (t + 1) * block]
        query_out[t, :, rank:] = rot_rows[t * block : (t + 1) * block]
    q_src = lambda to: query_out.at[to]
    q_dst = lambda i: query_in.at[i]
    exchange(1, q_src, q_dst)
    query_in[me] = query_out[me]
    if pairs > 2:
        hear()
        tell()

    kv_scale = lax.rsqrt(jnp.mean(kv_raw * kv_raw, axis=-1, keepdims=True) + EPS)
    loads[6].wait()
    latent_new = (kv_raw * kv_scale * kv_gain[...]).astype(BF)
    own_cols = pl.ds(pl.multiple_of(me * kc, kc), kc)
    latent_ref[...] = (kv_part.astype(F32) * kv_scale * kv_gain[:, own_cols]).astype(BF)
    latent_rows = mm(mine, latent_new)
    key_rows = mm(mine, key_new)
    loads[12].wait()

    arrive(1, q_src, q_dst)
    q_abs = jnp.concatenate([query_in[t, :, :rank] for t in range(tp_n)], axis=0)
    q_rot = jnp.concatenate([query_in[t, :, rank:] for t in range(tp_n)], axis=0)
    row_p, pos_p = iota((rows, positions), 0), iota((rows, positions), 1)
    row_seq = mod(row_p, s_here)
    scores = jnp.zeros((rows, positions), F32)
    for s in range(s_here):
        scores = jnp.where(row_seq == s, mm_nt(q_abs, cache[s]) + mm(q_rot, rotated[s]), scores)
    score_scale = qk ** (-0.5)
    scores = scores * score_scale
    self_score = (
        jnp.sum(q_abs.astype(F32) * latent_rows, axis=-1, keepdims=True)
        + jnp.sum(q_rot.astype(F32) * key_rows, axis=-1, keepdims=True)
    ) * score_scale
    valid = pos_p.astype(F32) < len_rows
    scores = jnp.where(valid, scores, -jnp.inf)
    top = jnp.maximum(jnp.max(scores, axis=-1, keepdims=True), self_score)
    weights = jnp.exp(scores - top)
    self_weight = jnp.exp(self_score - top)
    total = jnp.sum(weights, axis=-1, keepdims=True) + self_weight
    acc = self_weight.astype(BF).astype(F32) * latent_rows
    for s in range(s_here):
        acc = acc + mm(jnp.where(row_seq == s, weights, 0.0).astype(BF), cache[s])
    attended = (acc / total).astype(BF)
    for t in range(tp_n):
        att_out[t] = attended[t * block : (t + 1) * block]
    a_src = lambda to: att_out.at[to]
    a_dst = lambda i: att_in.at[i]
    exchange(2, a_src, a_dst)
    att_in[me] = att_out[me]

    def next_round(k, carry):
        hear()
        tell()
        return carry

    lax.fori_loop(2, pairs - 1, next_round, 0)
    loads[10].wait()
    loads[11].wait()
    seq_i, row_c = iota((seqs, rows), 0), iota((seqs, rows), 1)
    gather = jnp.where(div(row_c, block) * s_here + mod(row_c, s_here) == seq_i, 1.0, 0.0).astype(BF)

    arrive(2, a_src, a_dst)
    att = jnp.concatenate([att_in[t] for t in range(tp_n)], axis=0)
    values = jnp.where(head_lanes, mm(att, value_up[...]), 0.0).astype(BF)
    head_values = mm(gather, values).astype(BF)
    partial = mm(head_values, attn_out[...]).astype(BF)
    for t in range(tp_n):
        sum_out[t] = partial[:, t * cols : (t + 1) * cols]
    s_src = lambda to: sum_out.at[to]
    s_dst = lambda i: sum_in.at[i]
    exchange(3, s_src, s_dst)
    sum_in[me] = sum_out[me]
    if pairs > 1:
        hear()
    model_cols = pl.ds(pl.multiple_of(me * cols, cols), cols)
    tok_mine = tokens[:, model_cols].astype(F32)
    for i in (15, 16, 17, 18, 19, 20):
        loads[i].wait()
    eye_row = lambda row: jnp.sum(jnp.where(eye, row, 0.0), axis=1, keepdims=True)
    topk = route.shape[0]
    chosen = [eye_row(route[k : k + 1, :].astype(F32)) for k in range(topk)]
    chosen_weight = [eye_row(route_weight[k : k + 1, :]) for k in range(topk)]

    arrive(3, s_src, s_dst)
    head_sum = sum_in[0].astype(F32)
    for t in range(1, tp_n):
        head_sum = head_sum + sum_in[t].astype(F32)
    resid = (tok_mine + head_sum).astype(BF)
    rows_in[me, ep_me] = resid

    def rows_copy(origin, to):
        return pltpu.make_async_remote_copy(
            src_ref=rows_in.at[me, origin],
            dst_ref=rows_in.at[me, origin],
            send_sem=bulk.at[0],
            recv_sem=rows_recv.at[origin],
            device_id=(to, me),
            device_id_type=MESH,
        )

    low = lax.rem(me, 2)
    peers = [lax.rem(me - low + i, tp_n) for i in range(2, tp_n)] + [me + 1 - 2 * low]

    def pass_on(origin):
        for peer in peers:
            pltpu.make_async_remote_copy(
                src_ref=rows_in.at[me, origin],
                dst_ref=rows_in.at[me, origin],
                send_sem=bulk.at[1],
                recv_sem=bulk.at[2],
                device_id=(ep_me, peer),
                device_id_type=MESH,
            ).start()

    def at_distance(d, act):
        @pl.when(ep_me + d < ep_n)
        def _():
            act(ep_me + d)

        @pl.when(ep_me >= d)
        def _():
            act(ep_me - d)

    def farthest_first(act):
        def step(k, carry):
            at_distance(ep_n - k, act)
            return carry

        lax.fori_loop(1, ep_n, step, 0)

    def nearest_first(act):
        def step(k, carry):
            at_distance(k, act)
            return carry

        lax.fori_loop(1, ep_n, step, 0)

    farthest_first(lambda to: rows_copy(ep_me, to).start())
    pass_on(ep_me)

    def take_rows(origin):
        rows_copy(origin, origin).wait_recv()
        pass_on(origin)

    nearest_first(take_rows)

    def bulk_wait(ref, sem):
        return pltpu.make_async_copy(ref, ref, sem)

    most = rows_in.at[pl.ds(0, tp_n - 1)]
    bulk_wait(most, bulk.at[2]).wait()

    group = math.gcd(ep_n, 8)

    def expert(g, carry):
        first = g * group
        parts = []
        square = jnp.zeros((group * seqs, 1), F32)
        for t in range(tp_n):
            x = jnp.concatenate([rows_in[t, first + i] for i in range(group)], axis=0).astype(F32)
            square = square + jnp.sum(x * x, axis=-1, keepdims=True)
            parts.append(x)
        inverse = lax.rsqrt(square * (1.0 / (cols * tp_n)) + EPS)
        gate = jnp.zeros((group * seqs, gate_w.shape[2]), F32)
        up = jnp.zeros((group * seqs, gate_w.shape[2]), F32)
        for t in range(tp_n):
            here = slice(t * cols, (t + 1) * cols)
            x = (parts[t] * inverse * moe_gain[:, here]).astype(BF)
            gate = gate + mm(x, gate_w[0, here, :])
            up = up + mm(x, up_w[0, here, :])
        hidden = (gate / (1.0 + jnp.exp(-gate)) * up).astype(BF)
        for t in range(tp_n):
            here = slice(t * cols, (t + 1) * cols)
            part = mm(hidden, down_w[0, :, here]).astype(BF)
            for i in range(group):
                part_out[t, first + i] = part[i * seqs : (i + 1) * seqs]
        return carry

    if ep_n == group:
        expert(0, 0)
    else:
        lax.fori_loop(0, ep_n // group, expert, 0)

    def part_copy(to_tp, block_ep, origin):
        return pltpu.make_async_remote_copy(
            src_ref=part_out.at[to_tp, block_ep],
            dst_ref=part_in.at[origin, block_ep],
            send_sem=bulk.at[3],
            recv_sem=part_recv.at[block_ep, origin],
            device_id=(ep_me, to_tp),
            device_id_type=MESH,
        )

    def give_parts(block_ep):
        for peer in peers:
            part_copy(peer, block_ep, me).start()

    farthest_first(give_parts)
    give_parts(ep_me)

    def back_copy(to):
        return pltpu.make_async_remote_copy(
            src_ref=back_out.at[to],
            dst_ref=back_in.at[ep_me],
            send_sem=bulk.at[4],
            recv_sem=bulk.at[5],
            device_id=(to, me),
            device_id_type=MESH,
        )

    def summed(block_ep):
        found = part_out[me, block_ep].astype(F32)
        for j in range(1, tp_n):
            origin = lax.rem(me + j, tp_n)
            part_copy(origin, block_ep, origin).wait_recv()
            found = found + part_in[origin, block_ep].astype(F32)
        return found.astype(BF)

    def give_back(to):
        back_out[to] = summed(to)
        back_copy(to).start()

    farthest_first(give_back)
    back_in[ep_me] = summed(ep_me)

    def share_of(e):
        share = jnp.zeros((seqs, 1), F32)
        for k in range(topk):
            share = share + jnp.where(chosen[k] == jnp.float32(e), chosen_weight[k], 0.0)
        return share

    few = ep_n <= 8
    shares = [share_of(e) for e in range(ep_n)] if few else None
    bulk_wait(back_in.at[pl.ds(0, ep_n - 1)], bulk.at[5]).wait()
    mixed = jnp.zeros((seqs, cols), F32)
    if few:
        for e in range(ep_n):
            mixed = mixed + shares[e] * back_in[e].astype(F32)
    else:
        mixed = lax.fori_loop(
            0, ep_n, lambda e, m: m + share_of(lax.convert_element_type(e, F32)) * back_in[e].astype(F32), mixed
        )
    mixed_ref[...] = (resid.astype(F32) + mixed).astype(BF)

    sent(0, own_lat, lat_at)
    sent(1, q_src, q_dst)
    sent(2, a_src, a_dst)
    sent(3, s_src, s_dst)
    bulk_wait(back_out.at[pl.ds(0, ep_n - 1)], bulk.at[0]).wait()
    bulk_wait(most, bulk.at[1]).wait()
    bulk_wait(most, bulk.at[3]).wait()
    bulk_wait(back_out.at[pl.ds(0, ep_n - 1)], bulk.at[4]).wait()


def finish(a, b, c, x, y, z):
    x[...] = a[...]
    y[...] = b[...]
    z[...] = c[...]


def shards(ep_n, tp_n, *args):
    (
        tokens,
        attn_gain,
        q_down,
        kv_down,
        rope_down,
        q_latent_gain,
        kv_latent_gain,
        q_up,
        query_gain,
        key_up,
        value_up,
        attn_out,
        cache_latent,
        cache_rope,
        lengths,
        moe_gain,
        route,
        route_weight,
        expert_gate,
        expert_up,
        expert_down,
    ) = args
    assert expert_gate.shape[0] == 1 and ep_n % 2 == 0 and tp_n % 2 == 0
    row = lambda v: v.reshape(1, -1)
    operands = (
        tokens,
        row(attn_gain),
        q_down,
        kv_down,
        rope_down.T,
        row(q_latent_gain),
        row(kv_latent_gain),
        q_up.T,
        query_gain,
        key_up,
        value_up,
        attn_out,
        cache_latent,
        cache_rope,
        row(lengths),
        row(moe_gain),
        route.T,
        route_weight.T,
        expert_gate,
        expert_up,
        expert_down,
    )
    vmem = pl.BlockSpec(memory_space=pltpu.VMEM)
    anyspace = pl.BlockSpec(memory_space=pltpu.HBM)
    seqs, model = tokens.shape
    cols = model // tp_n
    n = ep_n * tp_n
    heads = query_gain.shape[0]
    s_here, _, rank = cache_latent.shape
    block = heads * s_here
    like = lambda v: pltpu.VMEM(v.shape, v.dtype)
    scratch = [like(v) for v in operands] + [
        pltpu.VMEM((tp_n, seqs, q_down.shape[1] + kv_down.shape[1]), BF),
        pltpu.VMEM((tp_n, block, rank + 128), BF),
        pltpu.VMEM((tp_n, block, rank + 128), BF),
        pltpu.VMEM((tp_n, block, rank), BF),
        pltpu.VMEM((tp_n, block, rank), BF),
        pltpu.VMEM((tp_n, seqs, cols), BF),
        pltpu.VMEM((tp_n, seqs, cols), BF),
        pltpu.VMEM((tp_n, ep_n, seqs, cols), BF),
        pltpu.VMEM((tp_n, ep_n, seqs, cols), BF),
        pltpu.VMEM((tp_n, ep_n, seqs, cols), BF),
        pltpu.VMEM((ep_n, seqs, cols), BF),
        pltpu.VMEM((ep_n, seqs, cols), BF),
        pltpu.SemaphoreType.DMA((len(operands),)),
        pltpu.SemaphoreType.DMA((4, tp_n)),
        pltpu.SemaphoreType.DMA((4, tp_n)),
        pltpu.SemaphoreType.DMA((ep_n,)),
        pltpu.SemaphoreType.DMA((ep_n, tp_n)),
        pltpu.SemaphoreType.DMA((6,)),
        pltpu.SemaphoreType.REGULAR((3,)),
    ]
    outs = (
        jax.ShapeDtypeStruct((seqs, cols), BF),
        jax.ShapeDtypeStruct((seqs, kv_down.shape[1]), BF),
        jax.ShapeDtypeStruct((seqs, rope_down.shape[1]), BF),
    )
    grant = 60 * 1024 * 1024
    found = pl.pallas_call(
        functools.partial(kernel, ep_n, tp_n, len(operands)),
        out_shape=outs,
        in_specs=[anyspace] * len(operands),
        out_specs=(vmem, vmem, vmem),
        scratch_shapes=scratch,
        compiler_params=pltpu.CompilerParams(collective_id=0, has_side_effects=True, vmem_limit_bytes=grant),
    )(*operands)
    return pl.pallas_call(finish, out_shape=outs, in_specs=[vmem] * 3, out_specs=(vmem, vmem, vmem), compiler_params=pltpu.CompilerParams(vmem_limit_bytes=grant))(*found)


def solution(mesh):
    placed = (
        P("ep", None),
        P(),
        P(None, "tp"),
        P(None, "tp"),
        P(),
        P(),
        P(),
        P(None, "tp"),
        P("tp", None),
        P(None, "tp"),
        P(None, "tp"),
        P("tp", None),
        P(("ep", "tp"), None, None),
        P(("ep", "tp"), None, None),
        P("ep"),
        P(),
        P("ep", None),
        P("ep", None),
        P("ep", None, "tp"),
        P("ep", None, "tp"),
        P("ep", "tp", None),
    )
    return jax.shard_map(
        functools.partial(shards, mesh.shape["ep"], mesh.shape["tp"]),
        mesh=mesh,
        in_specs=placed,
        out_specs=(P("ep", "tp"), P("ep", "tp"), P("ep", None)),
        check_vma=False,
    )
```
